32 devices in a mesh: fs: 8 (over z, x), tp: 4 (over y, core).
Axes of the slice: x: 2, y: 2, z: 4, core: 2. Of those that a mesh axis runs over, the one named last changes fastest.
Arguments:
- tokens: bfloat16 [8192, 2048], P('fs', 'tp'), may hold values from -6 to 6
- recurrence_norm_gain: float32 [2048], replicated, may hold values from 0.1 to 1.9
- output_gate_weight: bfloat16 [2048, 2816], P('fs', 'tp'), may hold values from -0.125 to 0.125
- recurrence_input_weight: bfloat16 [2048, 2816], P('fs', 'tp'), may hold values from -0.125 to 0.125
- convolution_taps: float32 [4, 2816], P(None, 'tp'), may hold values from -3 to 3
- recurrence_gate_weight: bfloat16 [8, 352, 352], P('tp'), may hold values from -0.3125 to 0.3125
- input_gate_weight: bfloat16 [8, 352, 352], P('tp'), may hold values from -0.3125 to 0.3125
- base_decay_logit: float32 [2816], P('tp'), may hold values from 4.5 to 9.5
- token_log_decay: float32 [8192], P('fs'), may hold values from -0.7 to 0, as said below
- recurrence_output_weight: bfloat16 [2816, 2048], P('tp', 'fs'), may hold values from -0.4375 to 0.4375
- feedforward_norm_gain: float32 [2048], replicated, may hold values from 0.1 to 1.9
- feedforward_gate_weight: bfloat16 [2048, 5632], P('fs', 'tp'), may hold values from -0.125 to 0.125
- feedforward_up_weight: bfloat16 [2048, 5632], P('fs', 'tp'), may hold values from -0.125 to 0.125
- feedforward_down_weight: bfloat16 [5632, 2048], P('tp', 'fs'), may hold values from -0.15625 to 0.15625
Outputs:
- layer_out: bfloat16 [8192, 2048], P('fs', 'tp')
The draws below stay inside these ranges and needn't reach their ends.
Inputs may be any that keep to these rules, and one draw needn't show every extreme that they name: `token_log_decay`: each entry is zero or lies between -0.7 and -0.22.
All inputs are finite; a program needn't handle non-finite values.
Results may differ from the reference program's by a relative error of at most 0.022.
Values may be sent and summed in bfloat16 or wider, within the bound.
A program may use at most 128 MiB of HBM per device.

```python
import jax
import jax.numpy as jnp
from jax import lax

D = 2048
R = 2816
BW = 352
FF = 5632
CONV = 4
LEN = 128
BLOCKS = 8
TOKENS = 8192
N_TP = 4


def draw_base_decay_logit(key, part):
    keys = jax.random.split(jax.random.fold_in(key, 11), 3)
    slower = jax.random.bernoulli(keys[0], 0.5, (R,))
    fast_values = jax.random.uniform(keys[1], (R,), jnp.float32, 4.5, 5.5)
    slow_values = jax.random.uniform(keys[2], (R,), jnp.float32, 6.5, 9.0)
    return jnp.where(slower, slow_values, fast_values)


def draw_token_log_decay(key, part):
    keys = jax.random.split(jax.random.fold_in(key, 23), 2)
    struck = jax.random.bernoulli(keys[0], 3.0 / LEN, (TOKENS,))
    depths = jax.random.uniform(keys[1], (TOKENS,), jnp.float32, -0.7, -0.22)
    return jnp.where(struck, depths, jnp.zeros((TOKENS,), jnp.float32))


def levels(stream_key, extent, shards, smallest, largest):
    loudness, own = 1.0, jax.random.fold_in(stream_key, 6)
    for axis_at, shards_of in shards:
        heights = jnp.exp(jax.random.uniform(jax.random.fold_in(own, axis_at), (shards_of,), jnp.float32, smallest / len(shards), largest / len(shards)))
        loudness = loudness * jnp.repeat(heights, extent[axis_at] // shards_of).reshape([-1 if axis == axis_at else 1 for axis in range(len(extent))])
    return loudness


def scatter_about(key, dims, deviation, limit, pieces=(), kind=jnp.bfloat16):
    entries = jax.random.normal(key, dims, jnp.float32) * deviation
    if len(pieces) > 0:
        entries = levels(key, dims, pieces, -0.22, 0.18) * entries
    return jnp.clip(entries, min=-limit, max=limit).astype(kind)


def setup_inputs(seed: int = 0) -> dict:
    arg_keys = jax.random.split(jax.random.key(seed), 15)
    return {
        "tokens": scatter_about(arg_keys[0], (TOKENS, D), 1.0, 6.0, ((0, 8), (1, 4))),
        "recurrence_norm_gain": jnp.clip(1.0 + 0.18 * jax.random.normal(arg_keys[1], (D,), jnp.float32), 0.1, 1.9),
        "output_gate_weight": scatter_about(arg_keys[2], (D, R), D ** -0.5, 0.125, ((0, 8), (1, 4))),
        "recurrence_input_weight": scatter_about(arg_keys[3], (D, R), D ** -0.5, 0.125, ((0, 8), (1, 4))),
        "convolution_taps": scatter_about(arg_keys[4], (CONV, R), CONV ** -0.5, 3.0, ((1, 4),), jnp.float32),
        "recurrence_gate_weight": scatter_about(arg_keys[5], (BLOCKS, BW, BW), BW ** -0.5, 0.3125, ((0, 4),)),
        "input_gate_weight": scatter_about(arg_keys[6], (BLOCKS, BW, BW), BW ** -0.5, 0.3125, ((0, 4),)),
        "base_decay_logit": draw_base_decay_logit(jax.random.fold_in(arg_keys[14], 71), 0),
        "token_log_decay": draw_token_log_decay(jax.random.fold_in(arg_keys[14], 71), 0),
        "recurrence_output_weight": scatter_about(arg_keys[9], (R, D), (R // 16) ** -0.5, 0.4375, ((0, 4), (1, 8))),
        "feedforward_norm_gain": jnp.clip(1.0 + 0.18 * jax.random.normal(arg_keys[10], (D,), jnp.float32), 0.1, 1.9),
        "feedforward_gate_weight": scatter_about(arg_keys[11], (D, FF), D ** -0.5, 0.125, ((0, 8), (1, 4))),
        "feedforward_up_weight": scatter_about(arg_keys[12], (D, FF), D ** -0.5, 0.125, ((0, 8), (1, 4))),
        "feedforward_down_weight": scatter_about(arg_keys[13], (FF, D), (FF // 4) ** -0.5, 0.15625, ((0, 4), (1, 8))),
    }


EPSILON = 1e-06
GATE_EXPONENT = 8.0

def norm_rows(values, gain_vec):
    widened = values.astype(jnp.float32)
    scaled = widened * lax.rsqrt(lax.optimization_barrier(jnp.mean(widened * widened, axis=-1, keepdims=True)) + EPSILON)
    return (scaled * gain_vec).astype(jnp.bfloat16)

def causal_taps(feature_vector, convolution_taps, length):
    row_count, channels = feature_vector.shape
    blocks = feature_vector.astype(jnp.float32).reshape(row_count // length, length, channels)
    tap_count = convolution_taps.shape[0]
    padded = jnp.pad(blocks, ((0, 0), (tap_count - 1, 0), (0, 0)))
    summed = jnp.zeros_like(blocks)
    for offset in range(tap_count):
        summed = summed + convolution_taps[offset] * padded[:, offset:offset + length]
    return summed.reshape(row_count, channels).astype(jnp.bfloat16)

def combine_steps(earlier, latter):
    return (earlier[0] * latter[0], latter[0] * earlier[1] + latter[1])

def linear_scan(decays, driven, length):
    row_count, channels = decays.shape
    shaped = (decays.reshape(row_count // length, length, channels), driven.reshape(row_count // length, length, channels))
    result = lax.associative_scan(combine_steps, shaped, axis=1)
    return result[1].reshape(row_count, channels)

def block_map(mixed_in, weight):
    row_count = mixed_in.shape[0]
    shaped = mixed_in.astype(jnp.float32).reshape(row_count, BLOCKS, BW)
    return jnp.einsum('tnd,nde->tne', shaped, weight.astype(jnp.float32)).reshape(row_count, R)

def grouped_product(values, weight, group_count):
    step_size = values.shape[1] // group_count
    summed = jnp.zeros((values.shape[0], weight.shape[1]), jnp.float32)
    for group_index in range(group_count):
        lower = group_index * step_size
        partial_product = jnp.dot(values[:, lower:lower + step_size], weight[lower:lower + step_size], preferred_element_type=jnp.float32).astype(jnp.bfloat16)
        summed = summed + lax.optimization_barrier(partial_product).astype(jnp.float32)
    return summed

def reference(tokens, recurrence_norm_gain, output_gate_weight, recurrence_input_weight, convolution_taps, recurrence_gate_weight, input_gate_weight, base_decay_logit, token_log_decay, recurrence_output_weight, feedforward_norm_gain, feedforward_gate_weight, feedforward_up_weight, feedforward_down_weight):
    normed = norm_rows(tokens, recurrence_norm_gain)
    gate_projected = jnp.dot(normed, output_gate_weight, preferred_element_type=jnp.float32)
    feature_vector = jnp.dot(normed, recurrence_input_weight, preferred_element_type=jnp.float32).astype(jnp.bfloat16)
    mixed_in = causal_taps(feature_vector, convolution_taps, LEN)
    recurrence_gate = jax.nn.sigmoid(block_map(mixed_in, recurrence_gate_weight))
    inject_gate = jax.nn.sigmoid(block_map(mixed_in, input_gate_weight))
    decay_log_value = -GATE_EXPONENT * jax.nn.softplus(-base_decay_logit)[None, :] * recurrence_gate + token_log_decay[:, None]
    decays = jnp.exp(decay_log_value)
    driven = jnp.sqrt(-jnp.expm1(2.0 * decay_log_value)) * (inject_gate * mixed_in.astype(jnp.float32))
    states = linear_scan(decays, driven, LEN)
    carried = (states * jax.nn.gelu(gate_projected)).astype(jnp.bfloat16)
    mixer_sum = grouped_product(carried, recurrence_output_weight, N_TP)
    residual = (tokens.astype(jnp.float32) + mixer_sum).astype(jnp.bfloat16)
    normed_two = norm_rows(residual, feedforward_norm_gain)
    gate_hidden = jnp.dot(normed_two, feedforward_gate_weight, preferred_element_type=jnp.float32)
    up_hidden = jnp.dot(normed_two, feedforward_up_weight, preferred_element_type=jnp.float32)
    hidden = (jax.nn.silu(gate_hidden) * up_hidden).astype(jnp.bfloat16)
    hidden_sum = grouped_product(hidden, feedforward_down_weight, N_TP)
    return (residual.astype(jnp.float32) + hidden_sum).astype(jnp.bfloat16)
```

```python
import functools

import jax
import jax.numpy as jnp
from jax import lax
from jax.experimental import pallas as pl
from jax.experimental.pallas import tpu as pltpu
from jax.sharding import PartitionSpec as P


LEN = 128
EPSILON = 1e-06
GATE_EXPONENT = 8.0


def ring_order(count):
    return tuple(range(0, count, 2)) + tuple(range(count - 1, 0, -2))


def ring_tables(count):
    order = ring_order(count)
    place = [0] * count
    for spot, index in enumerate(order):
        place[index] = spot
    shifts = [0]
    for step in range(1, count // 2):
        shifts += [-step, step]
    shifts.append(count // 2)
    table = [[order[(place[index] + shift) % count] for shift in shifts] for index in range(count)]
    return jnp.array(table, jnp.int32)[lax.axis_index("fs")]


def ring_gather(piece, count):
    order = ring_order(count)
    right = [(order[i], order[(i + 1) % count]) for i in range(count)]
    left = [(order[i], order[(i - 1) % count]) for i in range(count)]

    def hop(value, pairs):
        return lax.ppermute(value, "fs", pairs)

    found = [piece]
    forward = backward = piece
    half = count // 2
    for _ in range(1, half):
        forward = hop(forward, right)
        backward = hop(backward, left)
        found += [forward, backward]
    cut = piece.shape[0] // 2
    found.append(hop(forward[:cut], right))
    found.append(hop(backward[cut:], left))
    return found


def collect(owners_ref, pieces, whole_ref):
    rows = pieces[0].shape[1]
    for k, piece in enumerate(pieces[:-2]):
        spot = pl.ds(pl.multiple_of(owners_ref[k] * rows, rows), rows)
        for lead in range(2):
            whole_ref[lead, spot, :] = piece[lead]
    spot = pl.ds(pl.multiple_of(owners_ref[len(pieces) - 2] * rows, rows), rows)
    for lead in range(2):
        whole_ref[lead, spot, :] = pieces[len(pieces) - 2 + lead][0]


def norm_block(values_ref, gain_ref):
    widened = values_ref[...].astype(jnp.float32)
    scaled = widened * lax.rsqrt(jnp.mean(widened * widened, axis=-1, keepdims=True) + EPSILON)
    return (scaled * gain_ref[...]).astype(jnp.bfloat16)


ROWS = 2 * LEN
ORDERED = pltpu.CompilerParams(dimension_semantics=("arbitrary",), vmem_limit_bytes=60 * 1024 * 1024)


def once(shape):
    zeros = (0,) * len(shape)
    return pl.BlockSpec(shape, lambda i, *_: zeros, pipeline_mode=pl.Buffered(1))


def block_dense(weight):
    groups, block_width, _ = weight.shape
    identity = jnp.eye(groups, dtype=jnp.bfloat16)[:, None, :, None]
    return (weight[:, :, None, :] * identity).reshape(groups * block_width, groups * block_width)


def shift_down(values, amount, place, fill):
    return jnp.where(place >= amount, pltpu.roll(values, amount, 0), fill)


def mixer_kernel(owners_ref, rows_ref, gain_ref, taps_ref, recur_ref, inject_ref, rate_ref, token_ref, *rest):
    pieces, (out_ref, whole_ref) = rest[:-2], rest[-2:]

    @pl.when(pl.program_id(0) == 0)
    def _():
        collect(owners_ref, pieces, whole_ref)

    normed = norm_block(rows_ref, gain_ref)
    feature = jnp.dot(normed, whole_ref[1], preferred_element_type=jnp.float32)
    feature = feature.astype(jnp.bfloat16).astype(jnp.float32)
    place = lax.rem(lax.broadcasted_iota(jnp.int32, feature.shape, 0), LEN)
    taps = taps_ref[...]
    tap_count = taps.shape[0]
    summed = None
    for k in range(tap_count):
        amount = tap_count - 1 - k
        moved = shift_down(feature, amount, place, 0.0) if amount else feature
        term = taps[k : k + 1] * moved
        summed = term if summed is None else summed + term
    mixed = summed.astype(jnp.bfloat16)
    recur = jax.nn.sigmoid(jnp.dot(mixed, recur_ref[...], preferred_element_type=jnp.float32))
    inject = jax.nn.sigmoid(jnp.dot(mixed, inject_ref[...], preferred_element_type=jnp.float32))
    log_decay = rate_ref[...] * recur + token_ref[...]
    decay = jnp.exp(log_decay)
    y = 2.0 * log_decay
    series = -y * (
        1.0 + y * (1 / 2) * (1.0 + y * (1 / 3) * (1.0 + y * (1 / 4) * (1.0 + y * (1 / 5) * (1.0 + y * (1 / 6)))))
    )
    loss = jnp.where(y > -0.25, series, 1.0 - decay * decay)
    state = jnp.sqrt(loss) * (inject * mixed.astype(jnp.float32))
    amount = 1
    while amount < LEN:
        state = state + decay * shift_down(state, amount, place, 0.0)
        if 2 * amount < LEN:
            decay = decay * shift_down(decay, amount, place, 1.0)
        amount *= 2
    gate = jnp.dot(normed, whole_ref[0], preferred_element_type=jnp.float32)
    out_ref[...] = (state * jax.nn.gelu(gate)).astype(jnp.bfloat16)


def mixer(owners, full_rows, gain, taps, recur_weight, inject_weight, base_decay_logit, token_log_decay, pieces):
    rows, width = full_rows.shape
    channels = pieces[0].shape[-1]
    rate = -GATE_EXPONENT * jax.nn.softplus(-base_decay_logit)[None, :]
    block = lambda cols: pl.BlockSpec((ROWS, cols), lambda i, *_: (i, 0))
    return pl.pallas_call(
        mixer_kernel,
        grid_spec=pltpu.PrefetchScalarGridSpec(
            num_scalar_prefetch=1,
            grid=(rows // ROWS,),
            in_specs=[
                block(width),
                once((1, width)),
                once(taps.shape),
                once((channels, channels)),
                once((channels, channels)),
                once((1, channels)),
                block(1),
            ]
            + [once(piece.shape) for piece in pieces],
            out_specs=block(channels),
            scratch_shapes=[pltpu.VMEM((2, width, channels), jnp.bfloat16)],
        ),
        out_shape=jax.ShapeDtypeStruct((rows, channels), jnp.bfloat16),
        compiler_params=ORDERED,
        cost_estimate=pl.CostEstimate(
            flops=4 * rows * channels * (channels + width), bytes_accessed=4 * width * channels, transcendentals=0
        ),
    )(
        owners,
        full_rows,
        gain[None],
        taps,
        block_dense(recur_weight),
        block_dense(inject_weight),
        rate,
        token_log_decay[:, None],
        *pieces,
    )


def hidden_kernel(owners_ref, rows_ref, gain_ref, *rest):
    pieces, (out_ref, whole_ref) = rest[:-2], rest[-2:]

    @pl.when(pl.program_id(0) == 0)
    def _():
        collect(owners_ref, pieces, whole_ref)

    normed = norm_block(rows_ref, gain_ref)
    gate = jnp.dot(normed, whole_ref[0], preferred_element_type=jnp.float32)
    up = jnp.dot(normed, whole_ref[1], preferred_element_type=jnp.float32)
    out_ref[...] = (jax.nn.silu(gate) * up).astype(jnp.bfloat16)


def hidden_units(owners, full_rows, gain, pieces):
    rows, width = full_rows.shape
    units = pieces[0].shape[-1]
    block = lambda cols: pl.BlockSpec((ROWS, cols), lambda i, *_: (i, 0))
    return pl.pallas_call(
        hidden_kernel,
        grid_spec=pltpu.PrefetchScalarGridSpec(
            num_scalar_prefetch=1,
            grid=(rows // ROWS,),
            in_specs=[block(width), once((1, width))] + [once(piece.shape) for piece in pieces],
            out_specs=block(units),
            scratch_shapes=[pltpu.VMEM((2, width, units), jnp.bfloat16)],
        ),
        out_shape=jax.ShapeDtypeStruct((rows, units), jnp.bfloat16),
        compiler_params=ORDERED,
        cost_estimate=pl.CostEstimate(
            flops=4 * rows * units * width, bytes_accessed=4 * width * units, transcendentals=0
        ),
    )(owners, full_rows, gain[None], *pieces)


def down_kernel(groups, where_ref, values_ref, *rest):
    pieces, (mine_ref, other_ref) = rest[:-2], rest[-2:]
    values = values_ref[...]
    cols = pieces[0].shape[1]
    width = mine_ref.shape[2]
    y, core = where_ref[len(pieces)], where_ref[len(pieces) + 1]
    for k, piece in enumerate(pieces):
        term = jnp.dot(values, piece[...], preferred_element_type=jnp.float32).astype(jnp.bfloat16)
        start = where_ref[k] * cols
        target = start // width
        offset = pl.multiple_of(lax.rem(start, width), cols)
        turn = lax.rem(target // 2 - y + groups, groups)
        same = lax.rem(target, 2) == core

        @pl.when(same)
        def _():
            mine_ref[turn, :, pl.ds(offset, cols)] = term

        @pl.when(jnp.logical_not(same))
        def _():
            other_ref[turn, :, pl.ds(offset, cols)] = term


def project_down(owners, values, pieces, tp):
    rows, depth = values.shape
    cols = pieces[0].shape[1]
    width = cols * len(pieces) // tp
    groups = tp // 2
    tall = min(rows, 2 * ROWS)
    index = lax.axis_index("tp")
    where = jnp.concatenate([owners, jnp.stack([index // 2, index % 2]).astype(jnp.int32)])
    out_spec = pl.BlockSpec((groups, tall, width), lambda i, *_: (0, i, 0))
    shape = jax.ShapeDtypeStruct((groups, rows, width), jnp.bfloat16)
    return pl.pallas_call(
        functools.partial(down_kernel, groups),
        grid_spec=pltpu.PrefetchScalarGridSpec(
            num_scalar_prefetch=1,
            grid=(rows // tall,),
            in_specs=[pl.BlockSpec((tall, depth), lambda i, *_: (i, 0))] + [once(piece.shape) for piece in pieces],
            out_specs=[out_spec, out_spec],
        ),
        out_shape=[shape, shape],
        compiler_params=ORDERED,
        cost_estimate=pl.CostEstimate(
            flops=2 * rows * depth * cols * len(pieces), bytes_accessed=2 * depth * cols * len(pieces), transcendentals=0
        ),
    )(where, values, *pieces)


def scatter_sum(mine, other, tp):
    groups = tp // 2
    got = lax.ppermute(other, "tp", [(i, i ^ 1) for i in range(tp)])
    widen = lambda value: value.astype(jnp.float32)
    total = None
    for turn in range(1, groups):
        pair = (widen(mine[turn]) + widen(got[turn])).astype(jnp.bfloat16)
        perm = [(i, (i + 2 * turn) % tp) for i in range(tp)]
        arrived = widen(lax.ppermute(pair, "tp", perm))
        total = arrived if total is None else total + arrived
    own = widen(mine[0]) + widen(got[0])
    return own if total is None else own + total


def join_last(pieces):
    return pieces[:-2] + [jnp.concatenate(pieces[-2:], axis=0)]


def shards_general(
    count,
    tp,
    tokens,
    recurrence_norm_gain,
    output_gate_weight,
    recurrence_input_weight,
    convolution_taps,
    recurrence_gate_weight,
    input_gate_weight,
    base_decay_logit,
    token_log_decay,
    recurrence_output_weight,
    feedforward_norm_gain,
    feedforward_gate_weight,
    feedforward_up_weight,
    feedforward_down_weight,
):
    owners = ring_tables(count)
    first = ring_gather(jnp.stack([output_gate_weight, recurrence_input_weight]), count)
    out_pieces = join_last(ring_gather(recurrence_output_weight, count))
    second = ring_gather(jnp.stack([feedforward_gate_weight, feedforward_up_weight]), count)
    down_pieces = join_last(ring_gather(feedforward_down_weight, count))

    full_rows = lax.all_gather(tokens, "tp", axis=1, tiled=True)
    carried = mixer(
        owners,
        full_rows,
        recurrence_norm_gain,
        convolution_taps,
        recurrence_gate_weight,
        input_gate_weight,
        base_decay_logit,
        token_log_decay,
        first,
    )
    mine, other = project_down(owners, carried, out_pieces, tp)
    own_sum = scatter_sum(mine, other, tp)
    residual_own = (tokens.astype(jnp.float32) + own_sum).astype(jnp.bfloat16)
    residual_full = lax.all_gather(residual_own, "tp", axis=1, tiled=True)
    hidden = hidden_units(owners, residual_full, feedforward_norm_gain, second)
    chunks = 2 if hidden.shape[0] % (2 * ROWS) == 0 else 1
    size = hidden.shape[0] // chunks
    sums = []
    for chunk in range(chunks):
        mine, other = project_down(owners, hidden[chunk * size : (chunk + 1) * size], down_pieces, tp)
        sums.append(scatter_sum(mine, other, tp))
    own_down = jnp.concatenate(sums, axis=0)
    return (residual_own.astype(jnp.float32) + own_down).astype(jnp.bfloat16)


LANES = 128


def pad_lanes(values, width):
    return jnp.pad(values, [(0, 0)] * (values.ndim - 1) + [(0, width - values.shape[-1])])


def recurrence_block(prod, wide, taps, recur_w, inject_w, rate, token_col):
    gate = prod[:, :wide]
    feature = prod[:, wide:].astype(jnp.bfloat16).astype(jnp.float32)
    place = lax.rem(lax.broadcasted_iota(jnp.int32, feature.shape, 0), LEN)
    tap_count = taps.shape[0]
    summed = None
    for k in range(tap_count):
        amount = tap_count - 1 - k
        moved = shift_down(feature, amount, place, 0.0) if amount else feature
        term = taps[k : k + 1] * moved
        summed = term if summed is None else summed + term
    mixed = summed.astype(jnp.bfloat16)
    recur = jax.nn.sigmoid(jnp.dot(mixed, recur_w, preferred_element_type=jnp.float32))
    inject = jax.nn.sigmoid(jnp.dot(mixed, inject_w, preferred_element_type=jnp.float32))
    log_decay = rate * recur + token_col
    decay = jnp.exp(log_decay)
    y = 2.0 * log_decay
    series = -y * (
        1.0 + y * (1 / 2) * (1.0 + y * (1 / 3) * (1.0 + y * (1 / 4) * (1.0 + y * (1 / 5) * (1.0 + y * (1 / 6)))))
    )
    loss = jnp.where(y > -0.25, series, 1.0 - decay * decay)
    state = jnp.sqrt(loss) * (inject * mixed.astype(jnp.float32))
    amount = 1
    while amount < LEN:
        state = state + decay * shift_down(state, amount, place, 0.0)
        if 2 * amount < LEN:
            decay = decay * shift_down(decay, amount, place, 1.0)
        amount *= 2
    return (state * jax.nn.gelu(gate)).astype(jnp.bfloat16)


def layer_kernel(
    planes,
    tokens_ref,
    token_ref,
    first_ref,
    out_w_ref,
    second_ref,
    down_ref,
    gain_ref,
    gain_two_ref,
    taps_ref,
    recur_ref,
    inject_ref,
    rate_ref,
    result_ref,
    rows_ref,
    resid_ref,
    wf_ref,
    wo_ref,
    wg_ref,
    wd_ref,
    hid_ref,
    keep_ref,
    csend_ref,
    crecv_ref,
    xrecv_ref,
    ysend_ref,
    yrecv_ref,
    tokd_ref,
    local_sem,
    token_sem,
    wx_sem,
    wz_sem,
    wr_sem,
    ags_sem,
    agr_sem,
    cs_sem,
    cr_sem,
    xs_sem,
    xr_sem,
    ys_sem,
    yr_sem,
):
    fs, tp = lax.axis_index("fs"), lax.axis_index("tp")
    z, x = fs // 2, lax.rem(fs, 2)
    yy, c = tp // 2, lax.rem(tp, 2)
    ox, oy, oc = 1 - x, 1 - yy, 1 - c
    to_x, to_y, to_c = (z * 2 + ox, tp), (fs, oy * 2 + c), (fs, yy * 2 + oc)
    to_z = ((fs + 2, tp), (fs - 2, tp))
    last = planes - 1
    held, cols = tokens_ref.shape
    depth_rows = first_ref.shape[1]
    wide = wf_ref.shape[1] // 2
    chans = wo_ref.shape[0]
    units = wd_ref.shape[0]
    chunks = held // ROWS

    def mo(value, step):
        return pl.multiple_of(value, step)

    def remote(src, dst, send, recv, dest):
        return pltpu.make_async_remote_copy(
            src_ref=src, dst_ref=dst, send_sem=send, recv_sem=recv, device_id=dest, device_id_type=pl.DeviceIdType.MESH
        )

    sources = (first_ref, out_w_ref, second_ref, down_ref)

    def block(g, s):
        spot = pl.ds(mo(s * depth_rows, depth_rows), depth_rows)
        if g == 0:
            return wf_ref.at[spot, :]
        if g == 1:
            return wo_ref.at[:, spot]
        if g == 2:
            return wg_ref.at[spot, :]
        return wd_ref.at[:, spot]

    def z_copy(g, s, way, src=None):
        dst = block(g, s)
        return remote(dst if src is None else src, dst, wz_sem.at[way, g, s], wr_sem.at[g, s], to_z[way])

    def x_copy(g):
        return remote(sources[g].at[ox], block(g, fs), wx_sem.at[g], wr_sem.at[g, fs], to_x)

    def local_copy(g):
        return pltpu.make_async_copy(sources[g].at[x], block(g, fs), local_sem.at[g])

    def z_send(g, s, src=None):
        @pl.when(z < last)
        def _():
            z_copy(g, s, 0, src).start()

        @pl.when(z > 0)
        def _():
            z_copy(g, s, 1, src).start()

    def x_forward(g):
        s = z * 2 + ox
        z_copy(g, s, 0).wait_recv()
        z_send(g, s)

    def z_step(g, d):
        for side in (x, ox):

            @pl.when(z - d >= 0)
            def _():
                s = (z - d) * 2 + side
                z_copy(g, s, 0).wait_recv()

                @pl.when(z < last)
                def _():
                    z_copy(g, s, 0).start()

            @pl.when(z + d <= last)
            def _():
                s = (z + d) * 2 + side
                z_copy(g, s, 1).wait_recv()

                @pl.when(z > 0)
                def _():
                    z_copy(g, s, 1).start()

    def z_drain(g):
        x_copy(g).wait_send()
        for way in range(2):

            @pl.loop(0, 2 * planes)
            def _(s):
                sent = (s // 2 <= z) & (z < last) if way == 0 else (s // 2 >= z) & (z > 0)

                @pl.when(sent)
                def _():
                    z_copy(g, s, way).wait_send()

    def spread(buf, phase, k, slot, at, dest):
        xi, yi, ci = at
        where = buf.at[
            pl.ds(mo(xi * held + k * ROWS, ROWS), ROWS), pl.ds(mo((yi * 2 + ci) * cols, cols), cols)
        ]
        return remote(
            where, where, ags_sem.at[phase, k, slot], agr_sem.at[phase, k, xi * 4 + yi * 2 + ci], dest
        )

    own = (x, yy, c)

    def spread_own(buf, phase, k):
        spread(buf, phase, k, 0, own, to_x).start()
        spread(buf, phase, k, 1, own, to_y).start()
        spread(buf, phase, k, 2, own, to_c).start()

    def spread_x(buf, phase, k):
        at = (ox, yy, c)
        spread(buf, phase, k, 3, at, to_y).wait_recv()
        spread(buf, phase, k, 3, at, to_y).start()
        spread(buf, phase, k, 4, at, to_c).start()

    def spread_y(buf, phase, k):
        for slot, at in ((5, (x, oy, c)), (6, (ox, oy, c))):
            spread(buf, phase, k, slot, at, to_c).wait_recv()
            spread(buf, phase, k, slot, at, to_c).start()

    def spread_c(buf, phase, k):
        for xi in (x, ox):
            for yi in (yy, oy):
                spread(buf, phase, k, 2, (xi, yi, oc), to_c).wait_recv()

    def spread_drain(buf, phase, k):
        at_x = (ox, yy, c)
        spread(buf, phase, k, 0, own, to_x).wait_send()
        spread(buf, phase, k, 1, own, to_y).wait_send()
        spread(buf, phase, k, 2, own, to_c).wait_send()
        spread(buf, phase, k, 3, at_x, to_y).wait_send()
        spread(buf, phase, k, 4, at_x, to_c).wait_send()
        spread(buf, phase, k, 5, (x, oy, c), to_c).wait_send()
        spread(buf, phase, k, 6, (ox, oy, c), to_c).wait_send()

    def c_copy(j):
        return remote(csend_ref.at[j], crecv_ref.at[j], cs_sem.at[j], cr_sem.at[j], to_c)

    def x_sum_copy(j):
        return remote(keep_ref.at[j], xrecv_ref.at[j], xs_sem.at[j], xr_sem.at[j], to_x)

    def y_sum_copy(k):
        return remote(ysend_ref.at[k], yrecv_ref.at[k], ys_sem.at[k], yr_sem.at[k], to_y)

    def chunk_rows(j):
        side = jnp.where(j < chunks, ox, x)
        k = lax.rem(j, chunks)
        return side, k, pl.ds(mo(side * held + k * ROWS, ROWS), ROWS)

    def produce(j, left, weight_ref):
        for half in range(2):
            spot = pl.ds(mo((half * 2 + oc) * cols, cols), cols)
            part = jnp.dot(left, weight_ref[:, spot], preferred_element_type=jnp.float32)
            csend_ref[j, :, half * cols : (half + 1) * cols] = part.astype(jnp.bfloat16)
        for half in range(2):
            spot = pl.ds(mo((half * 2 + c) * cols, cols), cols)
            part = jnp.dot(left, weight_ref[:, spot], preferred_element_type=jnp.float32)
            keep_ref[j, :, half * cols : (half + 1) * cols] = part.astype(jnp.bfloat16)
        c_copy(j).start()

    def join_cores(j):
        c_copy(j).wait_recv()
        keep_ref[j] = (keep_ref[j].astype(jnp.float32) + crecv_ref[j].astype(jnp.float32)).astype(jnp.bfloat16)

        @pl.when(j < chunks)
        def _():
            x_sum_copy(j).start()

    def produce_all(make, weight_ref):
        @pl.loop(0, 2 * chunks)
        def _(j):
            produce(j, make(j), weight_ref)

            @pl.when(j > 0)
            def _():
                join_cores(j - 1)

        join_cores(2 * chunks - 1)

    def halves(k, side):
        spot = pl.ds(mo(side * cols, cols), cols)
        return keep_ref[chunks + k, :, spot].astype(jnp.float32) + xrecv_ref[k, :, spot].astype(jnp.float32)

    def join_x(k):
        x_sum_copy(k).wait_recv()
        ysend_ref[k] = halves(k, oy).astype(jnp.bfloat16)
        y_sum_copy(k).start()

    def join_y(k):
        y_sum_copy(k).wait_recv()
        return halves(k, yy) + yrecv_ref[k].astype(jnp.float32)

    def sums_drain():
        for j in range(2 * chunks):
            c_copy(j).wait_send()
        for k in range(chunks):
            x_sum_copy(k).wait_send()
            y_sum_copy(k).wait_send()

    own_cols = pl.ds(mo(tp * cols, cols), cols)

    def own_spot(k):
        return pl.ds(mo(x * held + k * ROWS, ROWS), ROWS)

    barrier = pltpu.get_barrier_semaphore()
    for dest in (to_x, to_y, to_c):
        pl.semaphore_signal(barrier, inc=1, device_id=dest, device_id_type=pl.DeviceIdType.MESH)

    @pl.when(z < last)
    def _():
        pl.semaphore_signal(barrier, inc=1, device_id=to_z[0], device_id_type=pl.DeviceIdType.MESH)

    @pl.when(z > 0)
    def _():
        pl.semaphore_signal(barrier, inc=1, device_id=to_z[1], device_id_type=pl.DeviceIdType.MESH)

    own_tokens = pltpu.make_async_copy(
        tokens_ref, rows_ref.at[pl.ds(mo(x * held, held), held), own_cols], token_sem.at[0]
    )
    own_decay = pltpu.make_async_copy(token_ref, tokd_ref.at[x], token_sem.at[1])
    sent_decay = remote(token_ref, tokd_ref.at[x], token_sem.at[2], token_sem.at[3], to_x)
    own_tokens.start()
    own_decay.start()
    for g in range(4):
        local_copy(g).start()
    pl.semaphore_wait(barrier, 3 + (z < last).astype(jnp.int32) + (z > 0).astype(jnp.int32))

    x_copy(0).start()
    z_send(0, fs, sources[0].at[x])
    sent_decay.start()
    own_tokens.wait()
    for k in range(chunks):
        spread_own(rows_ref, 0, k)
        if k == 0:
            x_copy(1).start()
    x_copy(2).start()
    x_copy(3).start()
    x_forward(0)
    z_step(0, 1)
    z_send(1, fs, sources[1].at[x])
    x_forward(1)
    for k in range(chunks):
        spread_x(rows_ref, 0, k)
    z_step(0, 2)
    z_step(1, 1)
    z_step(1, 2)
    z_send(2, fs, sources[2].at[x])
    for k in range(chunks):
        spread_y(rows_ref, 0, k)
    x_forward(2)
    for k in range(chunks):
        spread_c(rows_ref, 0, k)
    for g in range(4):
        local_copy(g).wait()
    own_decay.wait()
    sent_decay.wait()
    z_step(0, 3)
    z_step(1, 3)

    def mix(j):
        side, k, rows = chunk_rows(j)
        normed = norm_block(rows_ref.at[rows, :], gain_ref)
        prod = jnp.dot(normed, wf_ref[...], preferred_element_type=jnp.float32)
        columns = []
        for n in range(ROWS // LEN):
            line = tokd_ref[side, pl.ds(k * (ROWS // LEN) + n, 1), :]
            columns.append(jnp.transpose(jnp.broadcast_to(line, (LEN, LANES))))
        column = jnp.concatenate(columns, axis=0)
        column = jnp.concatenate([column] * (wide // LANES), axis=1)
        carried = recurrence_block(
            prod, wide, taps_ref[...], recur_ref[...], inject_ref[...], rate_ref[...], column
        )
        return carried[:, :chans]

    produce_all(mix, wo_ref)

    def residual_chunk(k):
        total = join_y(k) + rows_ref[own_spot(k), own_cols].astype(jnp.float32)
        resid_ref[own_spot(k), own_cols] = total.astype(jnp.bfloat16)
        spread_own(resid_ref, 1, k)

    join_x(0)
    z_step(2, 1)
    join_x(1)
    residual_chunk(0)
    join_x(2)
    residual_chunk(1)
    spread_x(resid_ref, 1, 0)
    join_x(3)
    residual_chunk(2)
    spread_x(resid_ref, 1, 1)
    residual_chunk(3)
    z_step(2, 2)
    z_send(3, fs, sources[3].at[x])
    x_forward(3)
    for k in range(2, chunks):
        spread_x(resid_ref, 1, k)
    for k in range(chunks):
        spread_y(resid_ref, 1, k)
    for k in range(chunks):
        spread_c(resid_ref, 1, k)
    sums_drain()
    z_step(2, 3)

    @pl.loop(0, 2 * chunks)
    def _(j):
        rows = pl.ds(mo(j * ROWS, ROWS), ROWS)
        normed = norm_block(resid_ref.at[rows, :], gain_two_ref)
        both = jnp.dot(normed, wg_ref[...], preferred_element_type=jnp.float32)
        hid_ref[rows, :] = (jax.nn.silu(both[:, :units]) * both[:, units:]).astype(jnp.bfloat16)

    z_step(3, 1)
    z_step(3, 2)
    z_step(3, 3)

    def lower(j):
        _, _, rows = chunk_rows(j)
        return hid_ref[rows, :]

    produce_all(lower, wd_ref)

    def result_chunk(k):
        total = join_y(k) + resid_ref[own_spot(k), own_cols].astype(jnp.float32)
        result_ref[k * ROWS : (k + 1) * ROWS, :] = total.astype(jnp.bfloat16)

    join_x(0)
    for k in range(1, chunks):
        join_x(k)
        result_chunk(k - 1)
    result_chunk(chunks - 1)

    sums_drain()
    for g in range(4):
        z_drain(g)
    for phase, buf in enumerate((rows_ref, resid_ref)):
        for k in range(chunks):
            spread_drain(buf, phase, k)


def shards_fused(
    count,
    tp,
    tokens,
    recurrence_norm_gain,
    output_gate_weight,
    recurrence_input_weight,
    convolution_taps,
    recurrence_gate_weight,
    input_gate_weight,
    base_decay_logit,
    token_log_decay,
    recurrence_output_weight,
    feedforward_norm_gain,
    feedforward_gate_weight,
    feedforward_up_weight,
    feedforward_down_weight,
):
    planes = count // 2
    x = lax.rem(lax.axis_index("fs"), 2)
    held, cols = tokens.shape
    width = cols * tp
    chans = output_gate_weight.shape[1] // 2
    units = feedforward_gate_weight.shape[1] // 2
    wide = -(-chans // LANES) * LANES
    chunks = held // ROWS

    def split(weight):
        return jnp.stack(jnp.split(weight, 2, axis=1))

    first = jnp.concatenate(
        [pad_lanes(split(output_gate_weight), wide), pad_lanes(split(recurrence_input_weight), wide)], axis=-1
    )
    second = jnp.concatenate([split(feedforward_gate_weight), split(feedforward_up_weight)], axis=-1)
    out_w = recurrence_output_weight.reshape(2, chans, -1)
    down = feedforward_down_weight.reshape(2, units, -1)
    half = lambda values, axis: lax.dynamic_slice_in_dim(values, x * chans, chans, axis)
    square = lambda weight: jnp.pad(weight[x], ((0, wide - chans), (0, wide - chans)))
    rate = -GATE_EXPONENT * jax.nn.softplus(-half(base_decay_logit, 0))[None, :]
    anywhere = pl.BlockSpec(memory_space=pl.ANY)
    inside = pl.BlockSpec(memory_space=pltpu.VMEM)
    bf16 = jnp.bfloat16
    copies = pltpu.SemaphoreType.DMA
    flops = 2 * 2 * held * (width * (2 * chans + 2 * units) + width * (chans + units))
    return pl.pallas_call(
        functools.partial(layer_kernel, planes),
        in_specs=[anywhere] * 6 + [inside] * 6,
        out_specs=inside,
        out_shape=jax.ShapeDtypeStruct((held, cols), bf16),
        scratch_shapes=[
            pltpu.VMEM((2 * held, width), bf16),
            pltpu.VMEM((2 * held, width), bf16),
            pltpu.VMEM((width, 2 * wide), bf16),
            pltpu.VMEM((chans, width), bf16),
            pltpu.VMEM((width, 2 * units), bf16),
            pltpu.VMEM((units, width), bf16),
            pltpu.VMEM((2 * held, units), bf16),
            pltpu.VMEM((2 * chunks, ROWS, 2 * cols), bf16),
            pltpu.VMEM((2 * chunks, ROWS, 2 * cols), bf16),
            pltpu.VMEM((2 * chunks, ROWS, 2 * cols), bf16),
            pltpu.VMEM((chunks, ROWS, 2 * cols), bf16),
            pltpu.VMEM((chunks, ROWS, cols), bf16),
            pltpu.VMEM((chunks, ROWS, cols), bf16),
            pltpu.VMEM((2, held // LEN, LEN), jnp.float32),
            copies((4,)),
            copies((4,)),
            copies((4,)),
            copies((2, 4, 2 * planes)),
            copies((4, 2 * planes)),
            copies((2, chunks, 7)),
            copies((2, chunks, 8)),
            copies((2 * chunks,)),
            copies((2 * chunks,)),
            copies((chunks,)),
            copies((chunks,)),
            copies((chunks,)),
            copies((chunks,)),
        ],
        compiler_params=pltpu.CompilerParams(
            collective_id=0, has_side_effects=True, vmem_limit_bytes=63 * 1024 * 1024
        ),
        cost_estimate=pl.CostEstimate(flops=flops, bytes_accessed=8 * held * width, transcendentals=0),
    )(
        tokens,
        token_log_decay.reshape(held // LEN, LEN),
        first,
        out_w,
        second,
        down,
        recurrence_norm_gain[None],
        feedforward_norm_gain[None],
        pad_lanes(half(convolution_taps, 1), wide),
        square(recurrence_gate_weight),
        square(input_gate_weight),
        pad_lanes(rate, wide),
    )


def solution(mesh):
    in_specs = (
        P("fs", "tp"),
        P(),
        P("fs", "tp"),
        P("fs", "tp"),
        P(None, "tp"),
        P("tp", None, None),
        P("tp", None, None),
        P("tp"),
        P("fs"),
        P("tp", "fs"),
        P(),
        P("fs", "tp"),
        P("fs", "tp"),
        P("tp", "fs"),
    )
    count, tp = mesh.shape["fs"], mesh.shape["tp"]
    if tp == 4:
        body = functools.partial(shards_fused, count, tp)
        return jax.shard_map(body, mesh=mesh, in_specs=in_specs, out_specs=P("fs", "tp"), check_vma=False)
    body = functools.partial(shards_general, count, tp)
    return jax.shard_map(body, mesh=mesh, in_specs=in_specs, out_specs=P("fs", "tp"), check_vma=False)
```

```python
import functools

import jax
import jax.numpy as jnp
from jax import lax
from jax.experimental import pallas as pl
from jax.experimental.pallas import tpu as pltpu
from jax.sharding import PartitionSpec as P


LEN = 128
EPSILON = 1e-06
GATE_EXPONENT = 8.0


def ring_order(count):
    return tuple(range(0, count, 2)) + tuple(range(count - 1, 0, -2))


def ring_tables(count):
    order = ring_order(count)
    place = [0] * count
    for spot, index in enumerate(order):
        place[index] = spot
    shifts = [0]
    for step in range(1, count // 2):
        shifts += [-step, step]
    shifts.append(count // 2)
    table = [[order[(place[index] + shift) % count] for shift in shifts] for index in range(count)]
    return jnp.array(table, jnp.int32)[lax.axis_index("fs")]


def ring_gather(piece, count):
    order = ring_order(count)
    right = [(order[i], order[(i + 1) % count]) for i in range(count)]
    left = [(order[i], order[(i - 1) % count]) for i in range(count)]

    def hop(value, pairs):
        return lax.ppermute(value, "fs", pairs)

    found = [piece]
    forward = backward = piece
    half = count // 2
    for _ in range(1, half):
        forward = hop(forward, right)
        backward = hop(backward, left)
        found += [forward, backward]
    cut = piece.shape[0] // 2
    found.append(hop(forward[:cut], right))
    found.append(hop(backward[cut:], left))
    return found


def collect(owners_ref, pieces, whole_ref):
    rows = pieces[0].shape[1]
    for k, piece in enumerate(pieces[:-2]):
        spot = pl.ds(pl.multiple_of(owners_ref[k] * rows, rows), rows)
        for lead in range(2):
            whole_ref[lead, spot, :] = piece[lead]
    spot = pl.ds(pl.multiple_of(owners_ref[len(pieces) - 2] * rows, rows), rows)
    for lead in range(2):
        whole_ref[lead, spot, :] = pieces[len(pieces) - 2 + lead][0]


def norm_block(values_ref, gain_ref):
    widened = values_ref[...].astype(jnp.float32)
    scaled = widened * lax.rsqrt(jnp.mean(widened * widened, axis=-1, keepdims=True) + EPSILON)
    return (scaled * gain_ref[...]).astype(jnp.bfloat16)


ROWS = 2 * LEN
ORDERED = pltpu.CompilerParams(dimension_semantics=("arbitrary",), vmem_limit_bytes=60 * 1024 * 1024)


def once(shape):
    zeros = (0,) * len(shape)
    return pl.BlockSpec(shape, lambda i, *_: zeros, pipeline_mode=pl.Buffered(1))


def block_dense(weight):
    groups, block_width, _ = weight.shape
    identity = jnp.eye(groups, dtype=jnp.bfloat16)[:, None, :, None]
    return (weight[:, :, None, :] * identity).reshape(groups * block_width, groups * block_width)


def shift_down(values, amount, place, fill):
    return jnp.where(place >= amount, pltpu.roll(values, amount, 0), fill)


def mixer_kernel(owners_ref, rows_ref, gain_ref, taps_ref, recur_ref, inject_ref, rate_ref, token_ref, *rest):
    pieces, (out_ref, whole_ref) = rest[:-2], rest[-2:]

    @pl.when(pl.program_id(0) == 0)
    def _():
        collect(owners_ref, pieces, whole_ref)

    normed = norm_block(rows_ref, gain_ref)
    feature = jnp.dot(normed, whole_ref[1], preferred_element_type=jnp.float32)
    feature = feature.astype(jnp.bfloat16).astype(jnp.float32)
    place = lax.rem(lax.broadcasted_iota(jnp.int32, feature.shape, 0), LEN)
    taps = taps_ref[...]
    tap_count = taps.shape[0]
    summed = None
    for k in range(tap_count):
        amount = tap_count - 1 - k
        moved = shift_down(feature, amount, place, 0.0) if amount else feature
        term = taps[k : k + 1] * moved
        summed = term if summed is None else summed + term
    mixed = summed.astype(jnp.bfloat16)
    recur = jax.nn.sigmoid(jnp.dot(mixed, recur_ref[...], preferred_element_type=jnp.float32))
    inject = jax.nn.sigmoid(jnp.dot(mixed, inject_ref[...], preferred_element_type=jnp.float32))
    log_decay = rate_ref[...] * recur + token_ref[...]
    decay = jnp.exp(log_decay)
    y = 2.0 * log_decay
    series = -y * (
        1.0 + y * (1 / 2) * (1.0 + y * (1 / 3) * (1.0 + y * (1 / 4) * (1.0 + y * (1 / 5) * (1.0 + y * (1 / 6)))))
    )
    loss = jnp.where(y > -0.25, series, 1.0 - decay * decay)
    state = jnp.sqrt(loss) * (inject * mixed.astype(jnp.float32))
    amount = 1
    while amount < LEN:
        state = state + decay * shift_down(state, amount, place, 0.0)
        if 2 * amount < LEN:
            decay = decay * shift_down(decay, amount, place, 1.0)
        amount *= 2
    gate = jnp.dot(normed, whole_ref[0], preferred_element_type=jnp.float32)
    out_ref[...] = (state * jax.nn.gelu(gate)).astype(jnp.bfloat16)


def mixer(owners, full_rows, gain, taps, recur_weight, inject_weight, base_decay_logit, token_log_decay, pieces):
    rows, width = full_rows.shape
    channels = pieces[0].shape[-1]
    rate = -GATE_EXPONENT * jax.nn.softplus(-base_decay_logit)[None, :]
    block = lambda cols: pl.BlockSpec((ROWS, cols), lambda i, *_: (i, 0))
    return pl.pallas_call(
        mixer_kernel,
        grid_spec=pltpu.PrefetchScalarGridSpec(
            num_scalar_prefetch=1,
            grid=(rows // ROWS,),
            in_specs=[
                block(width),
                once((1, width)),
                once(taps.shape),
                once((channels, channels)),
                once((channels, channels)),
                once((1, channels)),
                block(1),
            ]
            + [once(piece.shape) for piece in pieces],
            out_specs=block(channels),
            scratch_shapes=[pltpu.VMEM((2, width, channels), jnp.bfloat16)],
        ),
        out_shape=jax.ShapeDtypeStruct((rows, channels), jnp.bfloat16),
        compiler_params=ORDERED,
        cost_estimate=pl.CostEstimate(
            flops=4 * rows * channels * (channels + width), bytes_accessed=4 * width * channels, transcendentals=0
        ),
    )(
        owners,
        full_rows,
        gain[None],
        taps,
        block_dense(recur_weight),
        block_dense(inject_weight),
        rate,
        token_log_decay[:, None],
        *pieces,
    )


def hidden_kernel(owners_ref, rows_ref, gain_ref, *rest):
    pieces, (out_ref, whole_ref) = rest[:-2], rest[-2:]

    @pl.when(pl.program_id(0) == 0)
    def _():
        collect(owners_ref, pieces, whole_ref)

    normed = norm_block(rows_ref, gain_ref)
    gate = jnp.dot(normed, whole_ref[0], preferred_element_type=jnp.float32)
    up = jnp.dot(normed, whole_ref[1], preferred_element_type=jnp.float32)
    out_ref[...] = (jax.nn.silu(gate) * up).astype(jnp.bfloat16)


def hidden_units(owners, full_rows, gain, pieces):
    rows, width = full_rows.shape
    units = pieces[0].shape[-1]
    block = lambda cols: pl.BlockSpec((ROWS, cols), lambda i, *_: (i, 0))
    return pl.pallas_call(
        hidden_kernel,
        grid_spec=pltpu.PrefetchScalarGridSpec(
            num_scalar_prefetch=1,
            grid=(rows // ROWS,),
            in_specs=[block(width), once((1, width))] + [once(piece.shape) for piece in pieces],
            out_specs=block(units),
            scratch_shapes=[pltpu.VMEM((2, width, units), jnp.bfloat16)],
        ),
        out_shape=jax.ShapeDtypeStruct((rows, units), jnp.bfloat16),
        compiler_params=ORDERED,
        cost_estimate=pl.CostEstimate(
            flops=4 * rows * units * width, bytes_accessed=4 * width * units, transcendentals=0
        ),
    )(owners, full_rows, gain[None], *pieces)


def down_kernel(groups, where_ref, values_ref, *rest):
    pieces, (mine_ref, other_ref) = rest[:-2], rest[-2:]
    values = values_ref[...]
    cols = pieces[0].shape[1]
    width = mine_ref.shape[2]
    y, core = where_ref[len(pieces)], where_ref[len(pieces) + 1]
    for k, piece in enumerate(pieces):
        term = jnp.dot(values, piece[...], preferred_element_type=jnp.float32).astype(jnp.bfloat16)
        start = where_ref[k] * cols
        target = start // width
        offset = pl.multiple_of(lax.rem(start, width), cols)
        turn = lax.rem(target // 2 - y + groups, groups)
        same = lax.rem(target, 2) == core

        @pl.when(same)
        def _():
            mine_ref[turn, :, pl.ds(offset, cols)] = term

        @pl.when(jnp.logical_not(same))
        def _():
            other_ref[turn, :, pl.ds(offset, cols)] = term


def project_down(owners, values, pieces, tp):
    rows, depth = values.shape
    cols = pieces[0].shape[1]
    width = cols * len(pieces) // tp
    groups = tp // 2
    tall = min(rows, 2 * ROWS)
    index = lax.axis_index("tp")
    where = jnp.concatenate([owners, jnp.stack([index // 2, index % 2]).astype(jnp.int32)])
    out_spec = pl.BlockSpec((groups, tall, width), lambda i, *_: (0, i, 0))
    shape = jax.ShapeDtypeStruct((groups, rows, width), jnp.bfloat16)
    return pl.pallas_call(
        functools.partial(down_kernel, groups),
        grid_spec=pltpu.PrefetchScalarGridSpec(
            num_scalar_prefetch=1,
            grid=(rows // tall,),
            in_specs=[pl.BlockSpec((tall, depth), lambda i, *_: (i, 0))] + [once(piece.shape) for piece in pieces],
            out_specs=[out_spec, out_spec],
        ),
        out_shape=[shape, shape],
        compiler_params=ORDERED,
        cost_estimate=pl.CostEstimate(
            flops=2 * rows * depth * cols * len(pieces), bytes_accessed=2 * depth * cols * len(pieces), transcendentals=0
        ),
    )(where, values, *pieces)


def scatter_sum(mine, other, tp):
    groups = tp // 2
    got = lax.ppermute(other, "tp", [(i, i ^ 1) for i in range(tp)])
    widen = lambda value: value.astype(jnp.float32)
    total = None
    for turn in range(1, groups):
        pair = (widen(mine[turn]) + widen(got[turn])).astype(jnp.bfloat16)
        perm = [(i, (i + 2 * turn) % tp) for i in range(tp)]
        arrived = widen(lax.ppermute(pair, "tp", perm))
        total = arrived if total is None else total + arrived
    own = widen(mine[0]) + widen(got[0])
    return own if total is None else own + total


def join_last(pieces):
    return pieces[:-2] + [jnp.concatenate(pieces[-2:], axis=0)]


def shards_general(
    count,
    tp,
    tokens,
    recurrence_norm_gain,
    output_gate_weight,
    recurrence_input_weight,
    convolution_taps,
    recurrence_gate_weight,
    input_gate_weight,
    base_decay_logit,
    token_log_decay,
    recurrence_output_weight,
    feedforward_norm_gain,
    feedforward_gate_weight,
    feedforward_up_weight,
    feedforward_down_weight,
):
    owners = ring_tables(count)
    first = ring_gather(jnp.stack([output_gate_weight, recurrence_input_weight]), count)
    out_pieces = join_last(ring_gather(recurrence_output_weight, count))
    second = ring_gather(jnp.stack([feedforward_gate_weight, feedforward_up_weight]), count)
    down_pieces = join_last(ring_gather(feedforward_down_weight, count))

    full_rows = lax.all_gather(tokens, "tp", axis=1, tiled=True)
    carried = mixer(
        owners,
        full_rows,
        recurrence_norm_gain,
        convolution_taps,
        recurrence_gate_weight,
        input_gate_weight,
        base_decay_logit,
        token_log_decay,
        first,
    )
    mine, other = project_down(owners, carried, out_pieces, tp)
    own_sum = scatter_sum(mine, other, tp)
    residual_own = (tokens.astype(jnp.float32) + own_sum).astype(jnp.bfloat16)
    residual_full = lax.all_gather(residual_own, "tp", axis=1, tiled=True)
    hidden = hidden_units(owners, residual_full, feedforward_norm_gain, second)
    chunks = 2 if hidden.shape[0] % (2 * ROWS) == 0 else 1
    size = hidden.shape[0] // chunks
    sums = []
    for chunk in range(chunks):
        mine, other = project_down(owners, hidden[chunk * size : (chunk + 1) * size], down_pieces, tp)
        sums.append(scatter_sum(mine, other, tp))
    own_down = jnp.concatenate(sums, axis=0)
    return (residual_own.astype(jnp.float32) + own_down).astype(jnp.bfloat16)


LANES = 128


def pad_lanes(values, width):
    return jnp.pad(values, [(0, 0)] * (values.ndim - 1) + [(0, width - values.shape[-1])])


def recurrence_block(gate, feature, taps, recur_w, inject_w, rate, token_col):
    feature = feature.astype(jnp.bfloat16).astype(jnp.float32)
    place = lax.rem(lax.broadcasted_iota(jnp.int32, feature.shape, 0), LEN)
    tap_count = taps.shape[0]
    summed = None
    for k in range(tap_count):
        amount = tap_count - 1 - k
        moved = shift_down(feature, amount, place, 0.0) if amount else feature
        term = taps[k : k + 1] * moved
        summed = term if summed is None else summed + term
    mixed = summed.astype(jnp.bfloat16)
    recur = jax.nn.sigmoid(jnp.dot(mixed, recur_w, preferred_element_type=jnp.float32))
    inject = jax.nn.sigmoid(jnp.dot(mixed, inject_w, preferred_element_type=jnp.float32))
    log_decay = rate * recur + token_col
    decay = jnp.exp(log_decay)
    y = 2.0 * log_decay
    series = -y * (
        1.0 + y * (1 / 2) * (1.0 + y * (1 / 3) * (1.0 + y * (1 / 4) * (1.0 + y * (1 / 5) * (1.0 + y * (1 / 6)))))
    )
    loss = jnp.where(y > -0.25, series, 1.0 - decay * decay)
    state = jnp.sqrt(loss) * (inject * mixed.astype(jnp.float32))
    amount = 1
    while amount < LEN:
        state = state + decay * shift_down(state, amount, place, 0.0)
        if 2 * amount < LEN:
            decay = decay * shift_down(decay, amount, place, 1.0)
        amount *= 2
    return (state * jax.nn.gelu(gate)).astype(jnp.bfloat16)


def layer_kernel(
    planes,
    tokens_ref,
    token_ref,
    first_ref,
    out_w_ref,
    second_ref,
    down_ref,
    gain_ref,
    gain_two_ref,
    taps_ref,
    recur_ref,
    inject_ref,
    rate_ref,
    result_ref,
    rows_ref,
    resid_ref,
    wf_ref,
    wo_ref,
    wg_ref,
    wd_ref,
    hid_ref,
    keep_ref,
    csend_ref,
    crecv_ref,
    xrecv_ref,
    ysend_ref,
    yrecv_ref,
    tokd_ref,
    chan_ref,
    local_sem,
    token_sem,
    wx_sem,
    wz_sem,
    wr_sem,
    ags_sem,
    agr_sem,
    cs_sem,
    cr_sem,
    xs_sem,
    xr_sem,
    ys_sem,
    yr_sem,
    dcs_sem,
    dcr_sem,
    dxs_sem,
    dxr_sem,
    dys_sem,
    dyr_sem,
):
    fs, tp = lax.axis_index("fs"), lax.axis_index("tp")
    z, x = fs // 2, lax.rem(fs, 2)
    yy, c = tp // 2, lax.rem(tp, 2)
    ox, oy, oc = 1 - x, 1 - yy, 1 - c
    to_x, to_y, to_c = (z * 2 + ox, tp), (fs, oy * 2 + c), (fs, yy * 2 + oc)
    to_z = ((fs + 2, tp), (fs - 2, tp))
    last = planes - 1
    held, cols = tokens_ref.shape
    depth_rows = first_ref.shape[1]
    wide = wf_ref.shape[1] // 2
    chans = wo_ref.shape[0]
    units = wd_ref.shape[0]
    chunks = held // ROWS

    def mo(value, step):
        return pl.multiple_of(value, step)

    def remote(src, dst, send, recv, dest):
        return pltpu.make_async_remote_copy(
            src_ref=src, dst_ref=dst, send_sem=send, recv_sem=recv, device_id=dest, device_id_type=pl.DeviceIdType.MESH
        )

    sources = (first_ref, out_w_ref, second_ref, down_ref)

    def block(g, s):
        spot = pl.ds(mo(s * depth_rows, depth_rows), depth_rows)
        if g == 0:
            return wf_ref.at[spot, :]
        if g == 1:
            return wo_ref.at[:, spot]
        if g == 2:
            return wg_ref.at[spot, :]
        return wd_ref.at[:, spot]

    def z_copy(g, s, way, src=None):
        dst = block(g, s)
        return remote(dst if src is None else src, dst, wz_sem.at[way, g, s], wr_sem.at[g, s], to_z[way])

    def x_copy(g):
        return remote(sources[g].at[ox], block(g, fs), wx_sem.at[g], wr_sem.at[g, fs], to_x)

    def local_copy(g):
        return pltpu.make_async_copy(sources[g].at[x], block(g, fs), local_sem.at[g])

    def z_send(g, s, src=None):
        @pl.when(z < last)
        def _():
            z_copy(g, s, 0, src).start()

        @pl.when(z > 0)
        def _():
            z_copy(g, s, 1, src).start()

    def x_forward(g):
        s = z * 2 + ox
        z_copy(g, s, 0).wait_recv()
        z_send(g, s)

    def z_pass(g, d, sides):
        @pl.when((z > 0) & (z < last))
        def _():
            for side in sides:

                @pl.when(z - d >= 0)
                def _():
                    s = (z - d) * 2 + side
                    z_copy(g, s, 0).wait_recv()
                    z_copy(g, s, 0).start()

                @pl.when(z + d <= last)
                def _():
                    s = (z + d) * 2 + side
                    z_copy(g, s, 1).wait_recv()
                    z_copy(g, s, 1).start()

    def z_end(g, d, sides):
        for side in sides:

            @pl.when((z == last) & (z - d >= 0))
            def _():
                z_copy(g, (z - d) * 2 + side, 0).wait_recv()

            @pl.when((z == 0) & (z + d <= last))
            def _():
                z_copy(g, (z + d) * 2 + side, 1).wait_recv()

    def z_end_all(g):
        for d in range(1, planes):
            z_end(g, d, both)

    both = (x, ox)
    fixed = (0, 1)

    def z_drain(g):
        x_copy(g).wait_send()
        for way in range(2):

            @pl.loop(0, 2 * planes)
            def _(s):
                sent = (s // 2 <= z) & (z < last) if way == 0 else (s // 2 >= z) & (z > 0)

                @pl.when(sent)
                def _():
                    z_copy(g, s, way).wait_send()

    def spread(buf, phase, k, slot, at, dest):
        xi, yi, ci = at
        where = buf.at[
            pl.ds(mo(xi * held + k * ROWS, ROWS), ROWS), pl.ds(mo((yi * 2 + ci) * cols, cols), cols)
        ]
        return remote(
            where, where, ags_sem.at[phase, k, slot], agr_sem.at[phase, k, xi * 4 + yi * 2 + ci], dest
        )

    own = (x, yy, c)

    def spread_own(buf, phase, k):
        spread(buf, phase, k, 0, own, to_x).start()
        spread(buf, phase, k, 1, own, to_y).start()
        spread(buf, phase, k, 2, own, to_c).start()

    def routes(swap):
        over_x, over_y = (ox, yy, c), (x, oy, c)
        return (over_y, over_x, to_x) if swap else (over_x, over_y, to_y)

    def spread_on(buf, phase, k, swap):
        at, _, dest = routes(swap)
        spread(buf, phase, k, 3, at, dest).wait_recv()
        spread(buf, phase, k, 3, at, dest).start()
        spread(buf, phase, k, 4, at, to_c).start()

    def spread_rest(buf, phase, k, swap):
        _, other, _ = routes(swap)
        for slot, at in ((5, other), (6, (ox, oy, c))):
            spread(buf, phase, k, slot, at, to_c).wait_recv()
            spread(buf, phase, k, slot, at, to_c).start()

    def spread_c(buf, phase, k):
        for xi in (x, ox):
            for yi in (yy, oy):
                spread(buf, phase, k, 2, (xi, yi, oc), to_c).wait_recv()

    def spread_drain(buf, phase, k, swap):
        at, other, dest = routes(swap)
        spread(buf, phase, k, 0, own, to_x).wait_send()
        spread(buf, phase, k, 1, own, to_y).wait_send()
        spread(buf, phase, k, 2, own, to_c).wait_send()
        spread(buf, phase, k, 3, at, dest).wait_send()
        spread(buf, phase, k, 4, at, to_c).wait_send()
        spread(buf, phase, k, 5, other, to_c).wait_send()
        spread(buf, phase, k, 6, (ox, oy, c), to_c).wait_send()

    def tall(j):
        return pl.ds(mo(j * ROWS, ROWS), ROWS)

    def c_copy(j):
        return remote(csend_ref.at[tall(j), :], crecv_ref.at[tall(j), :], cs_sem.at[j], cr_sem.at[j], to_c)

    split = chunks // 2

    def side_cols(side):
        return pl.ds(mo(side * cols, cols), cols)

    def x_sum_copy(k):
        return remote(keep_ref.at[tall(k), :], xrecv_ref.at[tall(k), :], xs_sem.at[k], xr_sem.at[k], to_x)

    def y_sum_copy(k):
        return remote(ysend_ref.at[tall(k), :], yrecv_ref.at[tall(k), :], ys_sem.at[k], yr_sem.at[k], to_y)

    def y_own_copy(k):
        src = keep_ref.at[tall(chunks + k), side_cols(oy)]
        return remote(src, yrecv_ref.at[tall(k), :], ys_sem.at[k], yr_sem.at[k], to_y)

    def y_across_copy(k):
        src = keep_ref.at[tall(k), side_cols(oy)]
        return remote(src, ysend_ref.at[tall(k), :], ys_sem.at[chunks + k], yr_sem.at[chunks + k], to_y)

    def x_half_copy(k):
        spot = side_cols(yy)
        return remote(
            keep_ref.at[tall(k), spot], xrecv_ref.at[tall(k), spot], xs_sem.at[k], xr_sem.at[k], to_x
        )

    def chunk_rows(j):
        side = jnp.where(j < chunks, ox, x)
        k = lax.rem(j, chunks)
        return side, k, pl.ds(mo(side * held + k * ROWS, ROWS), ROWS)

    def produce(j, left, weight_ref):
        for half in range(2):
            spot = pl.ds(mo((half * 2 + oc) * cols, cols), cols)
            part = jnp.dot(left, weight_ref[:, spot], preferred_element_type=jnp.float32)
            csend_ref[tall(j), half * cols : (half + 1) * cols] = part.astype(jnp.bfloat16)
        for half in range(2):
            spot = pl.ds(mo((half * 2 + c) * cols, cols), cols)
            part = jnp.dot(left, weight_ref[:, spot], preferred_element_type=jnp.float32)
            keep_ref[tall(j), half * cols : (half + 1) * cols] = part.astype(jnp.bfloat16)
        c_copy(j).start()

    def join_cores(j):
        c_copy(j).wait_recv()
        keep_ref[tall(j), :] = (
            keep_ref[tall(j), :].astype(jnp.float32) + crecv_ref[tall(j), :].astype(jnp.float32)
        ).astype(jnp.bfloat16)

        @pl.when(j < split)
        def _():
            x_sum_copy(j).start()

        @pl.when((j >= split) & (j < chunks))
        def _():
            y_across_copy(j).start()

        @pl.when(j >= chunks + split)
        def _():
            y_own_copy(j - chunks).start()

    def turn(i):
        across = lax.rem(i, 2) * split + i // 2
        mine = chunks + lax.rem(i - chunks + split + chunks, chunks)
        return jnp.where(i < chunks, across, mine)

    def produce_all():
        @pl.loop(0, 2 * chunks)
        def _(i):
            j = turn(i)
            _, _, rows = chunk_rows(j)
            produce(j, hid_ref[rows, :chans], wo_ref)

            @pl.when(i > 0)
            def _():
                join_cores(turn(i - 1))

        join_cores(turn(2 * chunks - 1))

    def halves(k, side):
        spot = side_cols(side)
        return keep_ref[tall(chunks + k), spot].astype(jnp.float32) + xrecv_ref[tall(k), spot].astype(jnp.float32)

    def join_x(k):
        x_sum_copy(k).wait_recv()
        ysend_ref[tall(k), :] = halves(k, oy).astype(jnp.bfloat16)
        y_sum_copy(k).start()

    def join_across(k):
        y_across_copy(k).wait_recv()
        spot = side_cols(yy)
        keep_ref[tall(k), spot] = (
            keep_ref[tall(k), spot].astype(jnp.float32) + ysend_ref[tall(k), :].astype(jnp.float32)
        ).astype(jnp.bfloat16)
        x_half_copy(k).start()

    def join_y(k):
        if k < split:
            y_sum_copy(k).wait_recv()
        else:
            y_own_copy(k).wait_recv()
            x_half_copy(k).wait_recv()
        return halves(k, yy) + yrecv_ref[tall(k), :].astype(jnp.float32)

    def sums_drain():
        for j in range(2 * chunks):
            c_copy(j).wait_send()
        for k in range(chunks):
            if k < split:
                x_sum_copy(k).wait_send()
                y_sum_copy(k).wait_send()
            else:
                y_own_copy(k).wait_send()
                y_across_copy(k).wait_send()
                x_half_copy(k).wait_send()

    def near(n):
        orders = [sorted(range(planes), key=lambda other: (abs(other - p), other)) for p in range(planes)]
        found = orders[0][n]
        for p in range(1, planes):
            found = jnp.where(z == p, orders[p][n], found)
        return found

    x_rows = pl.ds(mo(ox * held, held), held)
    own_rows = pl.ds(mo(x * held, held), held)

    def wide_cols(zi, xi):
        return pl.ds(mo((zi * 2 + xi) * depth_rows, depth_rows), depth_rows)

    def slot_cols(zi, xi):
        return pl.ds(mo((zi // 2 * 2 + xi) * depth_rows, depth_rows), depth_rows)

    def down_c_copy(zi, xi, half):
        rows = own_rows if half else x_rows
        at = zi * 2 + xi
        return remote(
            rows_ref.at[rows, wide_cols(zi, xi)],
            crecv_ref.at[rows, slot_cols(zi, xi)],
            dcs_sem.at[half, at],
            dcr_sem.at[half, at],
            to_c,
        )

    def down_x_copy(zi, xi):
        at = zi * 2 + xi
        return remote(
            rows_ref.at[x_rows, wide_cols(zi, xi)],
            xrecv_ref.at[:, slot_cols(zi, xi)],
            dxs_sem.at[at],
            dxr_sem.at[at],
            to_x,
        )

    def down_y_copy(zi, xi):
        return remote(
            rows_ref.at[own_rows, wide_cols(zi, xi)],
            yrecv_ref.at[:, xi * depth_rows : (xi + 1) * depth_rows],
            dys_sem.at[xi],
            dyr_sem.at[xi],
            to_y,
        )

    def lower(zi, xi, half):
        rows = own_rows if half else x_rows
        part = jnp.dot(hid_ref[rows, :], wd_ref[:, wide_cols(zi, xi)], preferred_element_type=jnp.float32)
        rows_ref[rows, wide_cols(zi, xi)] = part.astype(jnp.bfloat16)

        @pl.when(lax.rem(zi, 2) == oc)
        def _():
            down_c_copy(zi, xi, half).start()

    def gather(zi, xi, half):
        @pl.when(lax.rem(zi, 2) == c)
        def _():
            rows = own_rows if half else x_rows
            down_c_copy(zi, xi, half).wait_recv()
            rows_ref[rows, wide_cols(zi, xi)] = (
                rows_ref[rows, wide_cols(zi, xi)].astype(jnp.float32)
                + crecv_ref[rows, slot_cols(zi, xi)].astype(jnp.float32)
            ).astype(jnp.bfloat16)
            if half == 0:
                down_x_copy(zi, xi).start()

    def both_x(zi, xi):
        return rows_ref[own_rows, wide_cols(zi, xi)].astype(jnp.float32) + xrecv_ref[:, slot_cols(zi, xi)].astype(
            jnp.float32
        )

    def down_join_x(zi, xi):
        @pl.when(lax.rem(zi, 2) == c)
        def _():
            down_x_copy(zi, xi).wait_recv()

            @pl.when(zi // 2 == oy)
            def _():
                rows_ref[own_rows, wide_cols(zi, xi)] = both_x(zi, xi).astype(jnp.bfloat16)
                down_y_copy(zi, xi).start()

    def down_last(zi, xi):
        @pl.when(zi == tp)
        def _():
            down_y_copy(zi, xi).wait_recv()
            spot = slice(xi * depth_rows, (xi + 1) * depth_rows)
            total = both_x(zi, xi) + yrecv_ref[:, spot].astype(jnp.float32)
            total = total + resid_ref[own_rows, wide_cols(zi, xi)].astype(jnp.float32)
            result_ref[:, spot] = total.astype(jnp.bfloat16)

    def down_drain(zi, xi):
        @pl.when(lax.rem(zi, 2) == oc)
        def _():
            for half in range(2):
                down_c_copy(zi, xi, half).wait_send()

        @pl.when(lax.rem(zi, 2) == c)
        def _():
            down_x_copy(zi, xi).wait_send()

            @pl.when(zi // 2 == oy)
            def _():
                down_y_copy(zi, xi).wait_send()

    own_cols = pl.ds(mo(tp * cols, cols), cols)

    def own_spot(k):
        return pl.ds(mo(x * held + k * ROWS, ROWS), ROWS)

    barrier = pltpu.get_barrier_semaphore()
    for dest in (to_x, to_y, to_c):
        pl.semaphore_signal(barrier, inc=1, device_id=dest, device_id_type=pl.DeviceIdType.MESH)

    @pl.when(z < last)
    def _():
        pl.semaphore_signal(barrier, inc=1, device_id=to_z[0], device_id_type=pl.DeviceIdType.MESH)

    @pl.when(z > 0)
    def _():
        pl.semaphore_signal(barrier, inc=1, device_id=to_z[1], device_id_type=pl.DeviceIdType.MESH)

    own_tokens = pltpu.make_async_copy(
        tokens_ref, rows_ref.at[pl.ds(mo(x * held, held), held), own_cols], token_sem.at[0]
    )
    own_decay = pltpu.make_async_copy(token_ref, tokd_ref.at[x], token_sem.at[1])
    sent_decay = remote(token_ref, tokd_ref.at[x], token_sem.at[2], token_sem.at[3], to_x)
    own_tokens.start()
    own_decay.start()
    for g in range(4):
        local_copy(g).start()
    pl.semaphore_wait(barrier, 3 + (z < last).astype(jnp.int32) + (z > 0).astype(jnp.int32))

    x_copy(0).start()
    z_send(0, fs, sources[0].at[x])
    z_send(1, fs, sources[1].at[x])
    sent_decay.start()
    own_tokens.wait()
    for k in range(chunks):
        spread_own(rows_ref, 0, k)
        if k == 0:
            x_copy(1).start()
    x_copy(2).start()
    x_copy(3).start()
    first_half = x == 0
    chan_ref[0 : taps_ref.shape[0], :] = jnp.where(first_half, taps_ref[:, :chans], taps_ref[:, chans:])
    chan_ref[taps_ref.shape[0] : taps_ref.shape[0] + 1, :] = jnp.where(
        first_half, rate_ref[:, :chans], rate_ref[:, chans:]
    )
    x_forward(0)
    z_pass(0, 1, both)
    for k in range(chunks):
        spread_on(rows_ref, 0, k, False)
    z_pass(0, 2, both)
    x_forward(1)
    z_pass(1, 1, both)
    for k in range(chunks):
        spread_rest(rows_ref, 0, k, False)
    for k in range(chunks):
        spread_c(rows_ref, 0, k)
    for g in range(4):
        local_copy(g).wait()
    own_decay.wait()
    sent_decay.wait()
    z_end_all(0)

    def mix(start):
        @pl.loop(start, start + chunks)
        def _(j):
            side, k, rows = chunk_rows(j)
            normed = norm_block(rows_ref.at[rows, :], gain_ref)
            prod = jnp.dot(normed, wf_ref[...], preferred_element_type=jnp.float32)
            columns = []
            for n in range(ROWS // LEN):
                line = tokd_ref[side, pl.ds(k * (ROWS // LEN) + n, 1), :]
                columns.append(jnp.transpose(jnp.broadcast_to(line, (LEN, LANES))))
            column = jnp.concatenate(columns, axis=0)
            column = jnp.concatenate([column] * (wide // LANES), axis=1)[:, :chans]
            taps = chan_ref[0 : taps_ref.shape[0], :]
            rate = chan_ref[taps_ref.shape[0] : taps_ref.shape[0] + 1, :]
            hid_ref[rows, :chans] = recurrence_block(
                prod[:, :chans], prod[:, wide : wide + chans], taps, recur_ref[x], inject_ref[x], rate, column
            )

    mix(0)
    z_pass(1, 2, both)
    z_send(2, fs, sources[2].at[x])
    x_forward(2)
    mix(chunks)
    z_end_all(1)
    produce_all()

    def residual_chunk(k):
        total = join_y(k) + rows_ref[own_spot(k), own_cols].astype(jnp.float32)
        resid_ref[own_spot(k), own_cols] = total.astype(jnp.bfloat16)
        spread_own(resid_ref, 1, k)

    for k in range(split, chunks):
        join_across(k)
    z_pass(2, 1, (x,))
    for k in range(split):
        join_x(k)
    z_pass(2, 1, (ox,))
    weave = [k + side for k in range(split) for side in (split, 0)]
    for k in weave:
        residual_chunk(k)
    z_pass(2, 2, (x,))
    for k in weave:
        spread_on(resid_ref, 1, k, k % 2 == 1)
    z_pass(2, 2, (ox,))
    z_copy(3, z * 2 + ox, 0).wait_recv()
    for xi in range(2):
        z_send(3, z * 2 + xi)
    for k in weave:
        spread_rest(resid_ref, 1, k, k % 2 == 1)
    for k in range(chunks):
        spread_c(resid_ref, 1, k)
    sums_drain()
    for k in range(chunks):
        spread_drain(rows_ref, 0, k, False)
    z_end_all(2)

    def hide(start):
        @pl.loop(start, start + chunks)
        def _(j):
            _, _, rows = chunk_rows(j)
            normed = norm_block(resid_ref.at[rows, :], gain_two_ref)
            pair = jnp.dot(normed, wg_ref[...], preferred_element_type=jnp.float32)
            hid_ref[rows, :] = (jax.nn.silu(pair[:, :units]) * pair[:, units:]).astype(jnp.bfloat16)

    def half_sums(n, half):
        for xi in range(2):
            lower(near(n), xi, half)
        for xi in range(2):
            gather(near(n), xi, half)

    def near_join(n):
        for xi in range(2):
            down_join_x(near(n), xi)

    def near_last(n):
        for xi in range(2):
            down_last(near(n), xi)

    hide(0)
    half_sums(0, 0)
    z_pass(3, 1, fixed)
    hide(chunks)
    half_sums(0, 1)
    z_pass(3, 2, fixed)
    z_end(3, 1, fixed)
    half_sums(1, 0)
    half_sums(1, 1)
    near_join(0)
    z_end(3, 2, fixed)
    half_sums(2, 0)
    half_sums(2, 1)
    near_join(1)
    for xi in range(2):
        z_end(3, 3, (xi,))
        lower(near(3), xi, 0)
        lower(near(3), xi, 1)
        gather(near(3), xi, 0)
        gather(near(3), xi, 1)
        if xi == 0:
            near_join(2)
    near_join(3)
    for n in range(planes):
        near_last(n)

    for n in range(planes):
        for xi in range(2):
            down_drain(near(n), xi)
    for g in range(4):
        z_drain(g)
    for k in range(chunks):
        spread_drain(resid_ref, 1, k, k % 2 == 1)


def shards_fused(
    count,
    tp,
    tokens,
    recurrence_norm_gain,
    output_gate_weight,
    recurrence_input_weight,
    convolution_taps,
    recurrence_gate_weight,
    input_gate_weight,
    base_decay_logit,
    token_log_decay,
    recurrence_output_weight,
    feedforward_norm_gain,
    feedforward_gate_weight,
    feedforward_up_weight,
    feedforward_down_weight,
):
    planes = count // 2
    held, cols = tokens.shape
    width = cols * tp
    chans = output_gate_weight.shape[1] // 2
    units = feedforward_gate_weight.shape[1] // 2
    wide = -(-chans // LANES) * LANES
    chunks = held // ROWS

    def split(weight):
        return jnp.stack(jnp.split(weight, 2, axis=1))

    first = jnp.concatenate(
        [pad_lanes(split(output_gate_weight), wide), pad_lanes(split(recurrence_input_weight), wide)], axis=-1
    )
    second = jnp.concatenate([split(feedforward_gate_weight), split(feedforward_up_weight)], axis=-1)
    out_w = recurrence_output_weight.reshape(2, chans, -1)
    down = feedforward_down_weight.reshape(2, units, -1)
    rate = -GATE_EXPONENT * jax.nn.softplus(-base_decay_logit)[None, :]
    anywhere = pl.BlockSpec(memory_space=pl.ANY)
    inside = pl.BlockSpec(memory_space=pltpu.VMEM)
    bf16 = jnp.bfloat16
    copies = pltpu.SemaphoreType.DMA
    flops = 2 * 2 * held * (width * (2 * chans + 2 * units) + width * (chans + units))
    return pl.pallas_call(
        functools.partial(layer_kernel, planes),
        in_specs=[anywhere] * 6 + [inside] * 6,
        out_specs=inside,
        out_shape=jax.ShapeDtypeStruct((held, cols), bf16),
        scratch_shapes=[
            pltpu.VMEM((2 * held, width), bf16),
            pltpu.VMEM((2 * held, width), bf16),
            pltpu.VMEM((width, 2 * wide), bf16),
            pltpu.VMEM((chans, width), bf16),
            pltpu.VMEM((width, 2 * units), bf16),
            pltpu.VMEM((units, width), bf16),
            pltpu.VMEM((2 * held, units), bf16),
            pltpu.VMEM((2 * held, 2 * cols), bf16),
            pltpu.VMEM((2 * held, 2 * cols), bf16),
            pltpu.VMEM((2 * held, 2 * cols), bf16),
            pltpu.VMEM((held, 2 * cols), bf16),
            pltpu.VMEM((held, cols), bf16),
            pltpu.VMEM((held, cols), bf16),
            pltpu.VMEM((2, held // LEN, LEN), jnp.float32),
            pltpu.VMEM((convolution_taps.shape[0] + 1, chans), jnp.float32),
            copies((4,)),
            copies((4,)),
            copies((4,)),
            copies((2, 4, 2 * planes)),
            copies((4, 2 * planes)),
            copies((2, chunks, 7)),
            copies((2, chunks, 8)),
            copies((2 * chunks,)),
            copies((2 * chunks,)),
            copies((chunks,)),
            copies((chunks,)),
            copies((2 * chunks,)),
            copies((2 * chunks,)),
            copies((2, 2 * planes)),
            copies((2, 2 * planes)),
            copies((2 * planes,)),
            copies((2 * planes,)),
            copies((2,)),
            copies((2,)),
        ],
        compiler_params=pltpu.CompilerParams(
            collective_id=0, has_side_effects=True, vmem_limit_bytes=63 * 1024 * 1024
        ),
        cost_estimate=pl.CostEstimate(flops=flops, bytes_accessed=8 * held * width, transcendentals=0),
    )(
        tokens,
        token_log_decay.reshape(held // LEN, LEN),
        first,
        out_w,
        second,
        down,
        recurrence_norm_gain[None],
        feedforward_norm_gain[None],
        convolution_taps,
        recurrence_gate_weight,
        input_gate_weight,
        rate,
    )


def solution(mesh):
    in_specs = (
        P("fs", "tp"),
        P(),
        P("fs", "tp"),
        P("fs", "tp"),
        P(None, "tp"),
        P("tp", None, None),
        P("tp", None, None),
        P("tp"),
        P("fs"),
        P("tp", "fs"),
        P(),
        P("fs", "tp"),
        P("fs", "tp"),
        P("tp", "fs"),
    )
    count, tp = mesh.shape["fs"], mesh.shape["tp"]
    if tp == 4:
        body = functools.partial(shards_fused, count, tp)
        return jax.shard_map(body, mesh=mesh, in_specs=in_specs, out_specs=P("fs", "tp"), check_vma=False)
    body = functools.partial(shards_general, count, tp)
    return jax.shard_map(body, mesh=mesh, in_specs=in_specs, out_specs=P("fs", "tp"), check_vma=False)
```

```python
import functools

import jax
import jax.numpy as jnp
from jax import lax
from jax.experimental import pallas as pl
from jax.experimental.pallas import tpu as pltpu
from jax.sharding import PartitionSpec as P


LEN = 128
EPSILON = 1e-06
GATE_EXPONENT = 8.0


def ring_order(count):
    return tuple(range(0, count, 2)) + tuple(range(count - 1, 0, -2))


def ring_tables(count):
    order = ring_order(count)
    place = [0] * count
    for spot, index in enumerate(order):
        place[index] = spot
    shifts = [0]
    for step in range(1, count // 2):
        shifts += [-step, step]
    shifts.append(count // 2)
    table = [[order[(place[index] + shift) % count] for shift in shifts] for index in range(count)]
    return jnp.array(table, jnp.int32)[lax.axis_index("fs")]


def ring_gather(piece, count):
    order = ring_order(count)
    right = [(order[i], order[(i + 1) % count]) for i in range(count)]
    left = [(order[i], order[(i - 1) % count]) for i in range(count)]

    def hop(value, pairs):
        return lax.ppermute(value, "fs", pairs)

    found = [piece]
    forward = backward = piece
    half = count // 2
    for _ in range(1, half):
        forward = hop(forward, right)
        backward = hop(backward, left)
        found += [forward, backward]
    cut = piece.shape[0] // 2
    found.append(hop(forward[:cut], right))
    found.append(hop(backward[cut:], left))
    return found


def collect(owners_ref, pieces, whole_ref):
    rows = pieces[0].shape[1]
    for k, piece in enumerate(pieces[:-2]):
        spot = pl.ds(pl.multiple_of(owners_ref[k] * rows, rows), rows)
        for lead in range(2):
            whole_ref[lead, spot, :] = piece[lead]
    spot = pl.ds(pl.multiple_of(owners_ref[len(pieces) - 2] * rows, rows), rows)
    for lead in range(2):
        whole_ref[lead, spot, :] = pieces[len(pieces) - 2 + lead][0]


def norm_block(values_ref, gain_ref):
    widened = values_ref[...].astype(jnp.float32)
    scaled = widened * lax.rsqrt(jnp.mean(widened * widened, axis=-1, keepdims=True) + EPSILON)
    return (scaled * gain_ref[...]).astype(jnp.bfloat16)


ROWS = 2 * LEN
ORDERED = pltpu.CompilerParams(dimension_semantics=("arbitrary",), vmem_limit_bytes=60 * 1024 * 1024)


def once(shape):
    zeros = (0,) * len(shape)
    return pl.BlockSpec(shape, lambda i, *_: zeros, pipeline_mode=pl.Buffered(1))


def block_dense(weight):
    groups, block_width, _ = weight.shape
    identity = jnp.eye(groups, dtype=jnp.bfloat16)[:, None, :, None]
    return (weight[:, :, None, :] * identity).reshape(groups * block_width, groups * block_width)


def shift_down(values, amount, place, fill):
    return jnp.where(place >= amount, pltpu.roll(values, amount, 0), fill)


def mixer_kernel(owners_ref, rows_ref, gain_ref, taps_ref, recur_ref, inject_ref, rate_ref, token_ref, *rest):
    pieces, (out_ref, whole_ref) = rest[:-2], rest[-2:]

    @pl.when(pl.program_id(0) == 0)
    def _():
        collect(owners_ref, pieces, whole_ref)

    normed = norm_block(rows_ref, gain_ref)
    feature = jnp.dot(normed, whole_ref[1], preferred_element_type=jnp.float32)
    feature = feature.astype(jnp.bfloat16).astype(jnp.float32)
    place = lax.rem(lax.broadcasted_iota(jnp.int32, feature.shape, 0), LEN)
    taps = taps_ref[...]
    tap_count = taps.shape[0]
    summed = None
    for k in range(tap_count):
        amount = tap_count - 1 - k
        moved = shift_down(feature, amount, place, 0.0) if amount else feature
        term = taps[k : k + 1] * moved
        summed = term if summed is None else summed + term
    mixed = summed.astype(jnp.bfloat16)
    recur = jax.nn.sigmoid(jnp.dot(mixed, recur_ref[...], preferred_element_type=jnp.float32))
    inject = jax.nn.sigmoid(jnp.dot(mixed, inject_ref[...], preferred_element_type=jnp.float32))
    log_decay = rate_ref[...] * recur + token_ref[...]
    decay = jnp.exp(log_decay)
    y = 2.0 * log_decay
    series = -y * (
        1.0 + y * (1 / 2) * (1.0 + y * (1 / 3) * (1.0 + y * (1 / 4) * (1.0 + y * (1 / 5) * (1.0 + y * (1 / 6)))))
    )
    loss = jnp.where(y > -0.25, series, 1.0 - decay * decay)
    state = jnp.sqrt(loss) * (inject * mixed.astype(jnp.float32))
    amount = 1
    while amount < LEN:
        state = state + decay * shift_down(state, amount, place, 0.0)
        if 2 * amount < LEN:
            decay = decay * shift_down(decay, amount, place, 1.0)
        amount *= 2
    gate = jnp.dot(normed, whole_ref[0], preferred_element_type=jnp.float32)
    out_ref[...] = (state * jax.nn.gelu(gate)).astype(jnp.bfloat16)


def mixer(owners, full_rows, gain, taps, recur_weight, inject_weight, base_decay_logit, token_log_decay, pieces):
    rows, width = full_rows.shape
    channels = pieces[0].shape[-1]
    rate = -GATE_EXPONENT * jax.nn.softplus(-base_decay_logit)[None, :]
    block = lambda cols: pl.BlockSpec((ROWS, cols), lambda i, *_: (i, 0))
    return pl.pallas_call(
        mixer_kernel,
        grid_spec=pltpu.PrefetchScalarGridSpec(
            num_scalar_prefetch=1,
            grid=(rows // ROWS,),
            in_specs=[
                block(width),
                once((1, width)),
                once(taps.shape),
                once((channels, channels)),
                once((channels, channels)),
                once((1, channels)),
                block(1),
            ]
            + [once(piece.shape) for piece in pieces],
            out_specs=block(channels),
            scratch_shapes=[pltpu.VMEM((2, width, channels), jnp.bfloat16)],
        ),
        out_shape=jax.ShapeDtypeStruct((rows, channels), jnp.bfloat16),
        compiler_params=ORDERED,
        cost_estimate=pl.CostEstimate(
            flops=4 * rows * channels * (channels + width), bytes_accessed=4 * width * channels, transcendentals=0
        ),
    )(
        owners,
        full_rows,
        gain[None],
        taps,
        block_dense(recur_weight),
        block_dense(inject_weight),
        rate,
        token_log_decay[:, None],
        *pieces,
    )


def hidden_kernel(owners_ref, rows_ref, gain_ref, *rest):
    pieces, (out_ref, whole_ref) = rest[:-2], rest[-2:]

    @pl.when(pl.program_id(0) == 0)
    def _():
        collect(owners_ref, pieces, whole_ref)

    normed = norm_block(rows_ref, gain_ref)
    gate = jnp.dot(normed, whole_ref[0], preferred_element_type=jnp.float32)
    up = jnp.dot(normed, whole_ref[1], preferred_element_type=jnp.float32)
    out_ref[...] = (jax.nn.silu(gate) * up).astype(jnp.bfloat16)


def hidden_units(owners, full_rows, gain, pieces):
    rows, width = full_rows.shape
    units = pieces[0].shape[-1]
    block = lambda cols: pl.BlockSpec((ROWS, cols), lambda i, *_: (i, 0))
    return pl.pallas_call(
        hidden_kernel,
        grid_spec=pltpu.PrefetchScalarGridSpec(
            num_scalar_prefetch=1,
            grid=(rows // ROWS,),
            in_specs=[block(width), once((1, width))] + [once(piece.shape) for piece in pieces],
            out_specs=block(units),
            scratch_shapes=[pltpu.VMEM((2, width, units), jnp.bfloat16)],
        ),
        out_shape=jax.ShapeDtypeStruct((rows, units), jnp.bfloat16),
        compiler_params=ORDERED,
        cost_estimate=pl.CostEstimate(
            flops=4 * rows * units * width, bytes_accessed=4 * width * units, transcendentals=0
        ),
    )(owners, full_rows, gain[None], *pieces)


def down_kernel(groups, where_ref, values_ref, *rest):
    pieces, (mine_ref, other_ref) = rest[:-2], rest[-2:]
    values = values_ref[...]
    cols = pieces[0].shape[1]
    width = mine_ref.shape[2]
    y, core = where_ref[len(pieces)], where_ref[len(pieces) + 1]
    for k, piece in enumerate(pieces):
        term = jnp.dot(values, piece[...], preferred_element_type=jnp.float32).astype(jnp.bfloat16)
        start = where_ref[k] * cols
        target = start // width
        offset = pl.multiple_of(lax.rem(start, width), cols)
        turn = lax.rem(target // 2 - y + groups, groups)
        same = lax.rem(target, 2) == core

        @pl.when(same)
        def _():
            mine_ref[turn, :, pl.ds(offset, cols)] = term

        @pl.when(jnp.logical_not(same))
        def _():
            other_ref[turn, :, pl.ds(offset, cols)] = term


def project_down(owners, values, pieces, tp):
    rows, depth = values.shape
    cols = pieces[0].shape[1]
    width = cols * len(pieces) // tp
    groups = tp // 2
    tall = min(rows, 2 * ROWS)
    index = lax.axis_index("tp")
    where = jnp.concatenate([owners, jnp.stack([index // 2, index % 2]).astype(jnp.int32)])
    out_spec = pl.BlockSpec((groups, tall, width), lambda i, *_: (0, i, 0))
    shape = jax.ShapeDtypeStruct((groups, rows, width), jnp.bfloat16)
    return pl.pallas_call(
        functools.partial(down_kernel, groups),
        grid_spec=pltpu.PrefetchScalarGridSpec(
            num_scalar_prefetch=1,
            grid=(rows // tall,),
            in_specs=[pl.BlockSpec((tall, depth), lambda i, *_: (i, 0))] + [once(piece.shape) for piece in pieces],
            out_specs=[out_spec, out_spec],
        ),
        out_shape=[shape, shape],
        compiler_params=ORDERED,
        cost_estimate=pl.CostEstimate(
            flops=2 * rows * depth * cols * len(pieces), bytes_accessed=2 * depth * cols * len(pieces), transcendentals=0
        ),
    )(where, values, *pieces)


def scatter_sum(mine, other, tp):
    groups = tp // 2
    got = lax.ppermute(other, "tp", [(i, i ^ 1) for i in range(tp)])
    widen = lambda value: value.astype(jnp.float32)
    total = None
    for turn in range(1, groups):
        pair = (widen(mine[turn]) + widen(got[turn])).astype(jnp.bfloat16)
        perm = [(i, (i + 2 * turn) % tp) for i in range(tp)]
        arrived = widen(lax.ppermute(pair, "tp", perm))
        total = arrived if total is None else total + arrived
    own = widen(mine[0]) + widen(got[0])
    return own if total is None else own + total


def join_last(pieces):
    return pieces[:-2] + [jnp.concatenate(pieces[-2:], axis=0)]


def shards_general(
    count,
    tp,
    tokens,
    recurrence_norm_gain,
    output_gate_weight,
    recurrence_input_weight,
    convolution_taps,
    recurrence_gate_weight,
    input_gate_weight,
    base_decay_logit,
    token_log_decay,
    recurrence_output_weight,
    feedforward_norm_gain,
    feedforward_gate_weight,
    feedforward_up_weight,
    feedforward_down_weight,
):
    owners = ring_tables(count)
    first = ring_gather(jnp.stack([output_gate_weight, recurrence_input_weight]), count)
    out_pieces = join_last(ring_gather(recurrence_output_weight, count))
    second = ring_gather(jnp.stack([feedforward_gate_weight, feedforward_up_weight]), count)
    down_pieces = join_last(ring_gather(feedforward_down_weight, count))

    full_rows = lax.all_gather(tokens, "tp", axis=1, tiled=True)
    carried = mixer(
        owners,
        full_rows,
        recurrence_norm_gain,
        convolution_taps,
        recurrence_gate_weight,
        input_gate_weight,
        base_decay_logit,
        token_log_decay,
        first,
    )
    mine, other = project_down(owners, carried, out_pieces, tp)
    own_sum = scatter_sum(mine, other, tp)
    residual_own = (tokens.astype(jnp.float32) + own_sum).astype(jnp.bfloat16)
    residual_full = lax.all_gather(residual_own, "tp", axis=1, tiled=True)
    hidden = hidden_units(owners, residual_full, feedforward_norm_gain, second)
    chunks = 2 if hidden.shape[0] % (2 * ROWS) == 0 else 1
    size = hidden.shape[0] // chunks
    sums = []
    for chunk in range(chunks):
        mine, other = project_down(owners, hidden[chunk * size : (chunk + 1) * size], down_pieces, tp)
        sums.append(scatter_sum(mine, other, tp))
    own_down = jnp.concatenate(sums, axis=0)
    return (residual_own.astype(jnp.float32) + own_down).astype(jnp.bfloat16)


LANES = 128
PIECES = 2


def recurrence_block(gate, feature, taps, recur_w, inject_w, rate, token_col):
    feature = feature.astype(jnp.bfloat16).astype(jnp.float32)
    place = lax.rem(lax.broadcasted_iota(jnp.int32, feature.shape, 0), LEN)
    tap_count = taps.shape[0]
    summed = None
    for k in range(tap_count):
        amount = tap_count - 1 - k
        moved = shift_down(feature, amount, place, 0.0) if amount else feature
        term = taps[k : k + 1] * moved
        summed = term if summed is None else summed + term
    mixed = summed.astype(jnp.bfloat16)
    recur = jax.nn.sigmoid(jnp.dot(mixed, recur_w, preferred_element_type=jnp.float32))
    inject = jax.nn.sigmoid(jnp.dot(mixed, inject_w, preferred_element_type=jnp.float32))
    log_decay = rate * recur + token_col
    decay = jnp.exp(log_decay)
    y = 2.0 * log_decay
    series = -y * (
        1.0 + y * (1 / 2) * (1.0 + y * (1 / 3) * (1.0 + y * (1 / 4) * (1.0 + y * (1 / 5) * (1.0 + y * (1 / 6)))))
    )
    loss = jnp.where(y > -0.25, series, 1.0 - decay * decay)
    state = jnp.sqrt(loss) * (inject * mixed.astype(jnp.float32))
    amount = 1
    while amount < LEN:
        state = state + decay * shift_down(state, amount, place, 0.0)
        if 2 * amount < LEN:
            decay = decay * shift_down(decay, amount, place, 1.0)
        amount *= 2
    return (state * jax.nn.gelu(gate)).astype(jnp.bfloat16)


def layer_kernel(
    planes,
    tokens_ref,
    token_ref,
    gate_in_ref,
    feature_in_ref,
    out_w_ref,
    gate_up_ref,
    up_ref,
    down_ref,
    gain_ref,
    gain_two_ref,
    taps_ref,
    recur_ref,
    inject_ref,
    rate_ref,
    result_ref,
    rows_ref,
    resid_ref,
    wf_ref,
    wo_ref,
    wg_ref,
    wd_ref,
    hid_ref,
    keep_ref,
    csend_ref,
    crecv_ref,
    xrecv_ref,
    ysend_ref,
    yrecv_ref,
    tokd_ref,
    chan_ref,
    local_sem,
    raw_sem,
    token_sem,
    wx_sem,
    wz_sem,
    wr_sem,
    ags_sem,
    agr_sem,
    cs_sem,
    cr_sem,
    xs_sem,
    xr_sem,
    ys_sem,
    yr_sem,
    dcs_sem,
    dcr_sem,
    dxs_sem,
    dxr_sem,
    dys_sem,
    dyr_sem,
):
    fs, tp = lax.axis_index("fs"), lax.axis_index("tp")
    z, x = fs // 2, lax.rem(fs, 2)
    yy, c = tp // 2, lax.rem(tp, 2)
    ox, oy, oc = 1 - x, 1 - yy, 1 - c
    here = (fs, tp)
    to_x, to_y, to_c = (z * 2 + ox, tp), (fs, oy * 2 + c), (fs, yy * 2 + oc)
    to_z = ((fs + 2, tp), (fs - 2, tp))
    last = planes - 1
    held, cols = tokens_ref.shape
    depth_rows = gate_in_ref.shape[2]
    chans = wo_ref.shape[0]
    units = wd_ref.shape[0]
    chunks = held // ROWS

    def mo(value, step):
        return pl.multiple_of(value, step)

    def remote(src, dst, send, recv, dest):
        return pltpu.make_async_remote_copy(
            src_ref=src, dst_ref=dst, send_sem=send, recv_sem=recv, device_id=dest, device_id_type=pl.DeviceIdType.MESH
        )

    staged = resid_ref.at[0:depth_rows, : 2 * units]
    raw = [resid_ref.at[n * depth_rows : (n + 1) * depth_rows, : 2 * units] for n in range(1, 3)]
    sources = (None, out_w_ref, None, down_ref)

    def block(g, s):
        spot = pl.ds(mo(s * depth_rows, depth_rows), depth_rows)
        if g == 0:
            return wf_ref.at[:, spot]
        if g == 1:
            return wo_ref.at[:, spot]
        if g == 2:
            return wg_ref.at[spot, :]
        return wd_ref.at[:, spot]

    def z_copy(g, s, way, src=None):
        dst = block(g, s)
        return remote(dst if src is None else src, dst, wz_sem.at[way, g, s], wr_sem.at[g, s], to_z[way])

    def x_copy(g):
        src = staged if g == 2 else sources[g].at[ox]
        return remote(src, block(g, fs), wx_sem.at[g], wr_sem.at[g, fs], to_x)

    projections = (gate_in_ref, feature_in_ref)

    def first_spot(n):
        return wf_ref.at[n * chans : (n + 1) * chans, pl.ds(mo(fs * depth_rows, depth_rows), depth_rows)]

    def first_x_copy(n):
        return remote(projections[n].at[ox], first_spot(n), wx_sem.at[4 * n], wr_sem.at[0, fs], to_x)

    def first_local_copy(n):
        return pltpu.make_async_copy(projections[n].at[x], first_spot(n), local_sem.at[2 * n])

    def local_copy(g):
        return pltpu.make_async_copy(sources[g].at[x], block(g, fs), local_sem.at[g])

    def z_send(g, s, src=None):
        @pl.when(z < last)
        def _():
            z_copy(g, s, 0, src).start()

        @pl.when(z > 0)
        def _():
            z_copy(g, s, 1, src).start()

    def x_forward(g):
        s = z * 2 + ox
        z_copy(g, s, 0).wait_recv()
        z_send(g, s)

    def z_pass(g, d, sides):
        @pl.when((z > 0) & (z < last))
        def _():
            for side in sides:

                @pl.when(z - d >= 0)
                def _():
                    s = (z - d) * 2 + side
                    z_copy(g, s, 0).wait_recv()
                    z_copy(g, s, 0).start()

                @pl.when(z + d <= last)
                def _():
                    s = (z + d) * 2 + side
                    z_copy(g, s, 1).wait_recv()
                    z_copy(g, s, 1).start()

    def z_end(g, d, sides):
        for side in sides:

            @pl.when((z == last) & (z - d >= 0))
            def _():
                z_copy(g, (z - d) * 2 + side, 0).wait_recv()

            @pl.when((z == 0) & (z + d <= last))
            def _():
                z_copy(g, (z + d) * 2 + side, 1).wait_recv()

    def z_end_all(g):
        for d in range(1, planes):
            z_end(g, d, both)

    both = (x, ox)
    fixed = (0, 1)

    def z_drain(g):
        for way in range(2):

            @pl.loop(0, 2 * planes)
            def _(s):
                sent = (s // 2 <= z) & (z < last) if way == 0 else (s // 2 >= z) & (z > 0)

                @pl.when(sent)
                def _():
                    z_copy(g, s, way).wait_send()

    def spread(buf, phase, k, slot, at, dest):
        xi, yi, ci = at
        where = buf.at[
            pl.ds(mo(xi * held + k * ROWS, ROWS), ROWS), pl.ds(mo((yi * 2 + ci) * cols, cols), cols)
        ]
        return remote(
            where, where, ags_sem.at[phase, k, slot], agr_sem.at[phase, k, xi * 4 + yi * 2 + ci], dest
        )

    own = (x, yy, c)

    def spread_own(buf, phase, k):
        spread(buf, phase, k, 0, own, to_x).start()
        spread(buf, phase, k, 1, own, to_y).start()
        spread(buf, phase, k, 2, own, to_c).start()

    def routes(swap):
        over_x, over_y = (ox, yy, c), (x, oy, c)
        return (over_y, over_x, to_x) if swap else (over_x, over_y, to_y)

    def spread_on(buf, phase, k, swap):
        at, _, dest = routes(swap)
        spread(buf, phase, k, 3, at, dest).wait_recv()
        spread(buf, phase, k, 3, at, dest).start()
        spread(buf, phase, k, 4, at, to_c).start()

    def spread_rest(buf, phase, k, swap):
        _, other, _ = routes(swap)
        for slot, at in ((5, other), (6, (ox, oy, c))):
            spread(buf, phase, k, slot, at, to_c).wait_recv()
            spread(buf, phase, k, slot, at, to_c).start()

    def spread_c(buf, phase, k):
        for xi in (x, ox):
            for yi in (yy, oy):
                spread(buf, phase, k, 2, (xi, yi, oc), to_c).wait_recv()

    def spread_drain(buf, phase, k, swap):
        at, other, dest = routes(swap)
        spread(buf, phase, k, 0, own, to_x).wait_send()
        spread(buf, phase, k, 1, own, to_y).wait_send()
        spread(buf, phase, k, 2, own, to_c).wait_send()
        spread(buf, phase, k, 3, at, dest).wait_send()
        spread(buf, phase, k, 4, at, to_c).wait_send()
        spread(buf, phase, k, 5, other, to_c).wait_send()
        spread(buf, phase, k, 6, (ox, oy, c), to_c).wait_send()

    def tall(j):
        return pl.ds(mo(j * ROWS, ROWS), ROWS)

    def c_copy(j):
        return remote(csend_ref.at[tall(j), :], crecv_ref.at[tall(j), :], cs_sem.at[j], cr_sem.at[j], to_c)

    split = chunks // 2

    def side_cols(side):
        return pl.ds(mo(side * cols, cols), cols)

    def x_sum_copy(k):
        return remote(keep_ref.at[tall(k), :], xrecv_ref.at[tall(k), :], xs_sem.at[k], xr_sem.at[k], to_x)

    def y_sum_copy(k):
        return remote(ysend_ref.at[tall(k), :], yrecv_ref.at[tall(k), :], ys_sem.at[k], yr_sem.at[k], to_y)

    def y_own_copy(k):
        src = keep_ref.at[tall(chunks + k), side_cols(oy)]
        return remote(src, yrecv_ref.at[tall(k), :], ys_sem.at[k], yr_sem.at[k], to_y)

    def y_across_copy(k):
        src = keep_ref.at[tall(k), side_cols(oy)]
        return remote(src, ysend_ref.at[tall(k), :], ys_sem.at[chunks + k], yr_sem.at[chunks + k], to_y)

    def x_half_copy(k):
        spot = side_cols(yy)
        return remote(
            keep_ref.at[tall(k), spot], xrecv_ref.at[tall(k), spot], xs_sem.at[k], xr_sem.at[k], to_x
        )

    def chunk_rows(j):
        side = jnp.where(j < chunks, ox, x)
        k = lax.rem(j, chunks)
        return side, k, pl.ds(mo(side * held + k * ROWS, ROWS), ROWS)

    def produce(j, left, weight_ref):
        for half in range(2):
            spot = pl.ds(mo((half * 2 + oc) * cols, cols), cols)
            part = jnp.dot(left, weight_ref[:, spot], preferred_element_type=jnp.float32)
            csend_ref[tall(j), half * cols : (half + 1) * cols] = part.astype(jnp.bfloat16)
        for half in range(2):
            spot = pl.ds(mo((half * 2 + c) * cols, cols), cols)
            part = jnp.dot(left, weight_ref[:, spot], preferred_element_type=jnp.float32)
            keep_ref[tall(j), half * cols : (half + 1) * cols] = part.astype(jnp.bfloat16)
        c_copy(j).start()

    def join_cores(j):
        c_copy(j).wait_recv()
        keep_ref[tall(j), :] = (
            keep_ref[tall(j), :].astype(jnp.float32) + crecv_ref[tall(j), :].astype(jnp.float32)
        ).astype(jnp.bfloat16)

        @pl.when(j < split)
        def _():
            x_sum_copy(j).start()

        @pl.when((j >= split) & (j < chunks))
        def _():
            y_across_copy(j).start()

        @pl.when(j >= chunks + split)
        def _():
            y_own_copy(j - chunks).start()

    def turn(i):
        across = lax.rem(i, 2) * split + i // 2
        mine = chunks + lax.rem(i - chunks + split + chunks, chunks)
        return jnp.where(i < chunks, across, mine)

    def produce_all():
        @pl.loop(0, 2 * chunks)
        def _(i):
            j = turn(i)
            _, _, rows = chunk_rows(j)
            produce(j, hid_ref[rows, :chans], wo_ref)

            @pl.when(i > 0)
            def _():
                join_cores(turn(i - 1))

        join_cores(turn(2 * chunks - 1))

    def halves(k, side):
        spot = side_cols(side)
        return keep_ref[tall(chunks + k), spot].astype(jnp.float32) + xrecv_ref[tall(k), spot].astype(jnp.float32)

    def join_x(k):
        x_sum_copy(k).wait_recv()
        ysend_ref[tall(k), :] = halves(k, oy).astype(jnp.bfloat16)
        y_sum_copy(k).start()

    def join_across(k):
        y_across_copy(k).wait_recv()
        spot = side_cols(yy)
        keep_ref[tall(k), spot] = (
            keep_ref[tall(k), spot].astype(jnp.float32) + ysend_ref[tall(k), :].astype(jnp.float32)
        ).astype(jnp.bfloat16)
        x_half_copy(k).start()

    def join_y(k):
        if k < split:
            y_sum_copy(k).wait_recv()
        else:
            y_own_copy(k).wait_recv()
            x_half_copy(k).wait_recv()
        return halves(k, yy) + yrecv_ref[tall(k), :].astype(jnp.float32)

    def sums_drain():
        for j in range(2 * chunks):
            c_copy(j).wait_send()
        for k in range(chunks):
            if k < split:
                x_sum_copy(k).wait_send()
                y_sum_copy(k).wait_send()
            else:
                y_own_copy(k).wait_send()
                y_across_copy(k).wait_send()
                x_half_copy(k).wait_send()

    def near(n):
        orders = [sorted(range(planes), key=lambda other: (abs(other - p), other)) for p in range(planes)]
        found = orders[0][n]
        for p in range(1, planes):
            found = jnp.where(z == p, orders[p][n], found)
        return found

    x_rows = pl.ds(mo(ox * held, held), held)
    own_rows = pl.ds(mo(x * held, held), held)

    def wide_cols(zi, xi):
        return pl.ds(mo((zi * 2 + xi) * depth_rows, depth_rows), depth_rows)

    def slot_cols(zi, xi):
        return pl.ds(mo((zi // 2 * 2 + xi) * depth_rows, depth_rows), depth_rows)

    def down_c_copy(zi, xi, half):
        rows = own_rows if half else x_rows
        at = zi * 2 + xi
        return remote(
            rows_ref.at[rows, wide_cols(zi, xi)],
            crecv_ref.at[rows, slot_cols(zi, xi)],
            dcs_sem.at[half, at],
            dcr_sem.at[half, at],
            to_c,
        )

    piece = held // PIECES

    def piece_rows(side, p):
        return pl.ds(mo(side * held + p * piece, piece), piece)

    def down_x_copy(zi, xi, p):
        at = zi * 2 + xi
        return remote(
            rows_ref.at[piece_rows(ox, p), wide_cols(zi, xi)],
            xrecv_ref.at[p * piece : (p + 1) * piece, slot_cols(zi, xi)],
            dxs_sem.at[p, at],
            dxr_sem.at[p, at],
            to_x,
        )

    def down_y_copy(zi, xi, p):
        return remote(
            rows_ref.at[piece_rows(x, p), wide_cols(zi, xi)],
            yrecv_ref.at[p * piece : (p + 1) * piece, xi * depth_rows : (xi + 1) * depth_rows],
            dys_sem.at[p, xi],
            dyr_sem.at[p, xi],
            to_y,
        )

    def lower(zi, xi, half):
        rows = own_rows if half else x_rows
        part = jnp.dot(hid_ref[rows, :], wd_ref[:, wide_cols(zi, xi)], preferred_element_type=jnp.float32)
        rows_ref[rows, wide_cols(zi, xi)] = part.astype(jnp.bfloat16)

        @pl.when(lax.rem(zi, 2) == oc)
        def _():
            down_c_copy(zi, xi, half).start()

    def gather(zi, xi, half):
        @pl.when(lax.rem(zi, 2) == c)
        def _():
            down_c_copy(zi, xi, half).wait_recv()
            for p in range(PIECES):
                rows = piece_rows(x if half else ox, p)
                rows_ref[rows, wide_cols(zi, xi)] = (
                    rows_ref[rows, wide_cols(zi, xi)].astype(jnp.float32)
                    + crecv_ref[rows, slot_cols(zi, xi)].astype(jnp.float32)
                ).astype(jnp.bfloat16)
                if half == 0:
                    down_x_copy(zi, xi, p).start()

    def both_x(zi, xi, p):
        mine = rows_ref[piece_rows(x, p), wide_cols(zi, xi)].astype(jnp.float32)
        return mine + xrecv_ref[p * piece : (p + 1) * piece, slot_cols(zi, xi)].astype(jnp.float32)

    def down_join_x(zi, xi):
        @pl.when(lax.rem(zi, 2) == c)
        def _():
            for p in range(PIECES):
                down_x_copy(zi, xi, p).wait_recv()

                @pl.when(zi // 2 == oy)
                def _():
                    rows_ref[piece_rows(x, p), wide_cols(zi, xi)] = both_x(zi, xi, p).astype(jnp.bfloat16)
                    down_y_copy(zi, xi, p).start()

    def down_last(zi, xi):
        @pl.when(zi == tp)
        def _():
            for p in range(PIECES):
                down_y_copy(zi, xi, p).wait_recv()
                rows = slice(p * piece, (p + 1) * piece)
                spot = slice(xi * depth_rows, (xi + 1) * depth_rows)
                total = both_x(zi, xi, p) + yrecv_ref[rows, spot].astype(jnp.float32)
                total = total + resid_ref[piece_rows(x, p), wide_cols(zi, xi)].astype(jnp.float32)
                result_ref[rows, spot] = total.astype(jnp.bfloat16)

    def down_drain(zi, xi):
        @pl.when(lax.rem(zi, 2) == oc)
        def _():
            for half in range(2):
                down_c_copy(zi, xi, half).wait_send()

        @pl.when(lax.rem(zi, 2) == c)
        def _():
            for p in range(PIECES):
                down_x_copy(zi, xi, p).wait_send()

            @pl.when(zi // 2 == oy)
            def _():
                for p in range(PIECES):
                    down_y_copy(zi, xi, p).wait_send()

    own_cols = pl.ds(mo(tp * cols, cols), cols)

    def own_spot(k):
        return pl.ds(mo(x * held + k * ROWS, ROWS), ROWS)

    barrier = pltpu.get_barrier_semaphore()
    for dest in (to_x, to_y, to_c):
        pl.semaphore_signal(barrier, inc=1, device_id=dest, device_id_type=pl.DeviceIdType.MESH)

    @pl.when(z < last)
    def _():
        pl.semaphore_signal(barrier, inc=1, device_id=to_z[0], device_id_type=pl.DeviceIdType.MESH)

    @pl.when(z > 0)
    def _():
        pl.semaphore_signal(barrier, inc=1, device_id=to_z[1], device_id_type=pl.DeviceIdType.MESH)

    own_tokens = pltpu.make_async_copy(
        tokens_ref, rows_ref.at[pl.ds(mo(x * held, held), held), own_cols], token_sem.at[0]
    )
    own_decay = pltpu.make_async_copy(token_ref, tokd_ref.at[x], token_sem.at[1])
    sent_decay = remote(token_ref, tokd_ref.at[x], token_sem.at[2], token_sem.at[3], to_x)
    own_tokens.start()
    own_decay.start()
    raws = [
        pltpu.make_async_copy(source, target, raw_sem.at[n])
        for n, (source, target) in enumerate(zip((gate_up_ref, up_ref), raw))
    ]
    for n in range(2):
        first_local_copy(n).start()
    for copy in raws:
        copy.start()
    for g in (1, 3):
        local_copy(g).start()
    first_half = x == 0

    def pick(values, here, width):
        left, right = values[:, :width], values[:, width:]
        return jnp.where(first_half == here, left, right)

    for n in range(2):
        first_local_copy(n).wait()
    pl.semaphore_wait(barrier, 3 + (z < last).astype(jnp.int32) + (z > 0).astype(jnp.int32))

    for n in range(2):
        first_x_copy(n).start()
    z_send(0, fs)
    z_send(1, fs, sources[1].at[x])
    sent_decay.start()
    own_tokens.wait()
    for k in range(chunks):
        spread_own(rows_ref, 0, k)
        if k == 0:
            x_copy(1).start()
    raws[0].wait()
    raws[1].wait()
    own_second = block(2, fs)
    for n in range(2):
        values = raw[n][...]
        for here, target in ((True, own_second), (False, staged)):
            target[:, n * units : (n + 1) * units] = pick(values, here, units)
    x_copy(2).start()
    x_copy(3).start()
    chan_ref[0 : taps_ref.shape[0], :] = jnp.where(first_half, taps_ref[:, :chans], taps_ref[:, chans:])
    chan_ref[taps_ref.shape[0] : taps_ref.shape[0] + 1, :] = jnp.where(
        first_half, rate_ref[:, :chans], rate_ref[:, chans:]
    )
    x_forward(0)
    z_pass(0, 1, both)
    for k in range(chunks):
        spread_on(rows_ref, 0, k, False)
    z_pass(0, 2, both)
    x_forward(1)
    z_pass(1, 1, both)
    for k in range(chunks):
        spread_rest(rows_ref, 0, k, False)
    for k in range(chunks):
        spread_c(rows_ref, 0, k)
    for g in (1, 3):
        local_copy(g).wait()
    own_decay.wait()
    sent_decay.wait()
    z_end_all(0)

    def mix(start):
        @pl.loop(start, start + chunks)
        def _(j):
            side, k, rows = chunk_rows(j)
            normed = norm_block(rows_ref.at[rows, :], gain_ref)
            prod = lax.dot_general(
                normed, wf_ref[...], (((1,), (1,)), ((), ())), preferred_element_type=jnp.float32
            )
            columns = []
            for n in range(ROWS // LEN):
                line = tokd_ref[side, pl.ds(k * (ROWS // LEN) + n, 1), :]
                columns.append(jnp.transpose(jnp.broadcast_to(line, (LEN, LANES))))
            column = jnp.concatenate(columns, axis=0)
            column = jnp.concatenate([column] * (-(-chans // LANES)), axis=1)[:, :chans]
            taps = chan_ref[0 : taps_ref.shape[0], :]
            rate = chan_ref[taps_ref.shape[0] : taps_ref.shape[0] + 1, :]
            hid_ref[rows, :chans] = recurrence_block(
                prod[:, :chans], prod[:, chans:], taps, recur_ref[x], inject_ref[x], rate, column
            )

    mix(0)
    z_pass(1, 2, both)
    z_send(2, fs)
    x_forward(2)
    mix(chunks)
    z_end_all(1)
    x_copy(2).wait_send()
    produce_all()

    def residual_chunk(k):
        total = join_y(k) + rows_ref[own_spot(k), own_cols].astype(jnp.float32)
        resid_ref[own_spot(k), own_cols] = total.astype(jnp.bfloat16)
        spread_own(resid_ref, 1, k)

    for k in range(split, chunks):
        join_across(k)
    z_pass(2, 1, (x,))
    for k in range(split):
        join_x(k)
    z_pass(2, 1, (ox,))
    weave = [k + side for k in range(split) for side in (split, 0)]
    for k in weave:
        residual_chunk(k)
    z_pass(2, 2, (x,))
    for k in weave:
        spread_on(resid_ref, 1, k, k % 2 == 1)
    z_pass(2, 2, (ox,))
    for k in weave:
        spread_rest(resid_ref, 1, k, k % 2 == 1)
    for k in range(chunks):
        spread_c(resid_ref, 1, k)
    z_copy(3, z * 2 + ox, 0).wait_recv()
    for xi in range(2):
        z_send(3, z * 2 + xi)
    sums_drain()
    for k in range(chunks):
        spread_drain(rows_ref, 0, k, False)
    z_end_all(2)

    def hide(start, stop):
        @pl.loop(start, stop)
        def _(j):
            _, _, rows = chunk_rows(j)
            normed = norm_block(resid_ref.at[rows, :], gain_two_ref)
            pair = jnp.dot(normed, wg_ref[...], preferred_element_type=jnp.float32)
            hid_ref[rows, :] = (jax.nn.silu(pair[:, :units]) * pair[:, units:]).astype(jnp.bfloat16)

    def half_sums(n, half):
        for xi in range(2):
            lower(near(n), xi, half)
        for xi in range(2):
            gather(near(n), xi, half)

    def near_join(n):
        for xi in range(2):
            down_join_x(near(n), xi)

    def near_last(n):
        for xi in range(2):
            down_last(near(n), xi)

    hide(0, chunks)
    half_sums(0, 0)
    z_pass(3, 1, fixed)
    hide(chunks, chunks + split)
    z_end(3, 1, fixed)
    half_sums(1, 0)
    hide(chunks + split, 2 * chunks)
    half_sums(0, 1)
    half_sums(1, 1)
    near_join(0)
    z_pass(3, 2, fixed)
    z_end(3, 2, fixed)
    half_sums(2, 0)
    half_sums(2, 1)
    near_join(1)
    for xi in range(2):
        z_end(3, 3, (xi,))
        lower(near(3), xi, 0)
        lower(near(3), xi, 1)
        gather(near(3), xi, 0)
        gather(near(3), xi, 1)
        if xi == 0:
            near_join(2)
    near_join(3)
    for n in range(planes):
        near_last(n)

    for n in range(planes):
        for xi in range(2):
            down_drain(near(n), xi)
    for n in range(2):
        first_x_copy(n).wait_send()
    for g in (1, 3):
        x_copy(g).wait_send()
    for g in range(4):
        z_drain(g)
    for k in range(chunks):
        spread_drain(resid_ref, 1, k, k % 2 == 1)


def shards_fused(
    count,
    tp,
    tokens,
    recurrence_norm_gain,
    output_gate_weight,
    recurrence_input_weight,
    convolution_taps,
    recurrence_gate_weight,
    input_gate_weight,
    base_decay_logit,
    token_log_decay,
    recurrence_output_weight,
    feedforward_norm_gain,
    feedforward_gate_weight,
    feedforward_up_weight,
    feedforward_down_weight,
):
    planes = count // 2
    held, cols = tokens.shape
    width = cols * tp
    chans = output_gate_weight.shape[1] // 2
    units = feedforward_gate_weight.shape[1] // 2
    chunks = held // ROWS

    out_w = recurrence_output_weight.reshape(2, chans, -1)
    down = feedforward_down_weight.reshape(2, units, -1)
    rate = -GATE_EXPONENT * jax.nn.softplus(-base_decay_logit)[None, :]
    anywhere = pl.BlockSpec(memory_space=pl.ANY)
    inside = pl.BlockSpec(memory_space=pltpu.VMEM)
    bf16 = jnp.bfloat16
    copies = pltpu.SemaphoreType.DMA
    flops = 2 * 2 * held * (width * (2 * chans + 2 * units) + width * (chans + units))
    return pl.pallas_call(
        functools.partial(layer_kernel, planes),
        in_specs=[anywhere] * 8 + [inside] * 6,
        out_specs=inside,
        out_shape=jax.ShapeDtypeStruct((held, cols), bf16),
        scratch_shapes=[
            pltpu.VMEM((2 * held, width), bf16),
            pltpu.VMEM((2 * held, width), bf16),
            pltpu.VMEM((2 * chans, width), bf16),
            pltpu.VMEM((chans, width), bf16),
            pltpu.VMEM((width, 2 * units), bf16),
            pltpu.VMEM((units, width), bf16),
            pltpu.VMEM((2 * held, units), bf16),
            pltpu.VMEM((2 * held, 2 * cols), bf16),
            pltpu.VMEM((2 * held, 2 * cols), bf16),
            pltpu.VMEM((2 * held, 2 * cols), bf16),
            pltpu.VMEM((held, 2 * cols), bf16),
            pltpu.VMEM((held, cols), bf16),
            pltpu.VMEM((held, cols), bf16),
            pltpu.VMEM((2, held // LEN, LEN), jnp.float32),
            pltpu.VMEM((convolution_taps.shape[0] + 1, chans), jnp.float32),
            copies((4,)),
            copies((2,)),
            copies((4,)),
            copies((5,)),
            copies((2, 4, 2 * planes)),
            copies((4, 2 * planes)),
            copies((2, chunks, 7)),
            copies((2, chunks, 8)),
            copies((2 * chunks,)),
            copies((2 * chunks,)),
            copies((chunks,)),
            copies((chunks,)),
            copies((2 * chunks,)),
            copies((2 * chunks,)),
            copies((2, 2 * planes)),
            copies((2, 2 * planes)),
            copies((PIECES, 2 * planes)),
            copies((PIECES, 2 * planes)),
            copies((PIECES, 2)),
            copies((PIECES, 2)),
        ],
        compiler_params=pltpu.CompilerParams(
            collective_id=0, has_side_effects=True, vmem_limit_bytes=63 * 1024 * 1024
        ),
        cost_estimate=pl.CostEstimate(flops=flops, bytes_accessed=8 * held * width, transcendentals=0),
    )(
        tokens,
        token_log_decay.reshape(held // LEN, LEN),
        output_gate_weight.T.reshape(2, chans, -1),
        recurrence_input_weight.T.reshape(2, chans, -1),
        out_w,
        feedforward_gate_weight,
        feedforward_up_weight,
        down,
        recurrence_norm_gain[None],
        feedforward_norm_gain[None],
        convolution_taps,
        recurrence_gate_weight,
        input_gate_weight,
        rate,
    )


def solution(mesh):
    in_specs = (
        P("fs", "tp"),
        P(),
        P("fs", "tp"),
        P("fs", "tp"),
        P(None, "tp"),
        P("tp", None, None),
        P("tp", None, None),
        P("tp"),
        P("fs"),
        P("tp", "fs"),
        P(),
        P("fs", "tp"),
        P("fs", "tp"),
        P("tp", "fs"),
    )
    count, tp = mesh.shape["fs"], mesh.shape["tp"]
    if tp == 4:
        body = functools.partial(shards_fused, count, tp)
        return jax.shard_map(body, mesh=mesh, in_specs=in_specs, out_specs=P("fs", "tp"), check_vma=False)
    body = functools.partial(shards_general, count, tp)
    return jax.shard_map(body, mesh=mesh, in_specs=in_specs, out_specs=P("fs", "tp"), check_vma=False)
```

```python
import functools

import jax
import jax.numpy as jnp
from jax import lax
from jax.experimental import pallas as pl
from jax.experimental.pallas import tpu as pltpu
from jax.sharding import PartitionSpec as P


LEN = 128
EPSILON = 1e-06
GATE_EXPONENT = 8.0


def ring_order(count):
    return tuple(range(0, count, 2)) + tuple(range(count - 1, 0, -2))


def ring_tables(count):
    order = ring_order(count)
    place = [0] * count
    for spot, index in enumerate(order):
        place[index] = spot
    shifts = [0]
    for step in range(1, count // 2):
        shifts += [-step, step]
    shifts.append(count // 2)
    table = [[order[(place[index] + shift) % count] for shift in shifts] for index in range(count)]
    return jnp.array(table, jnp.int32)[lax.axis_index("fs")]


def ring_gather(piece, count):
    order = ring_order(count)
    right = [(order[i], order[(i + 1) % count]) for i in range(count)]
    left = [(order[i], order[(i - 1) % count]) for i in range(count)]

    def hop(value, pairs):
        return lax.ppermute(value, "fs", pairs)

    found = [piece]
    forward = backward = piece
    half = count // 2
    for _ in range(1, half):
        forward = hop(forward, right)
        backward = hop(backward, left)
        found += [forward, backward]
    cut = piece.shape[0] // 2
    found.append(hop(forward[:cut], right))
    found.append(hop(backward[cut:], left))
    return found


def collect(owners_ref, pieces, whole_ref):
    rows = pieces[0].shape[1]
    for k, piece in enumerate(pieces[:-2]):
        spot = pl.ds(pl.multiple_of(owners_ref[k] * rows, rows), rows)
        for lead in range(2):
            whole_ref[lead, spot, :] = piece[lead]
    spot = pl.ds(pl.multiple_of(owners_ref[len(pieces) - 2] * rows, rows), rows)
    for lead in range(2):
        whole_ref[lead, spot, :] = pieces[len(pieces) - 2 + lead][0]


def norm_block(values_ref, gain_ref):
    widened = values_ref[...].astype(jnp.float32)
    scaled = widened * lax.rsqrt(jnp.mean(widened * widened, axis=-1, keepdims=True) + EPSILON)
    return (scaled * gain_ref[...]).astype(jnp.bfloat16)


ROWS = 2 * LEN
ORDERED = pltpu.CompilerParams(dimension_semantics=("arbitrary",), vmem_limit_bytes=60 * 1024 * 1024)


def once(shape):
    zeros = (0,) * len(shape)
    return pl.BlockSpec(shape, lambda i, *_: zeros, pipeline_mode=pl.Buffered(1))


def block_dense(weight):
    groups, block_width, _ = weight.shape
    identity = jnp.eye(groups, dtype=jnp.bfloat16)[:, None, :, None]
    return (weight[:, :, None, :] * identity).reshape(groups * block_width, groups * block_width)


def shift_down(values, amount, place, fill):
    return jnp.where(place >= amount, pltpu.roll(values, amount, 0), fill)


def mixer_kernel(owners_ref, rows_ref, gain_ref, taps_ref, recur_ref, inject_ref, rate_ref, token_ref, *rest):
    pieces, (out_ref, whole_ref) = rest[:-2], rest[-2:]

    @pl.when(pl.program_id(0) == 0)
    def _():
        collect(owners_ref, pieces, whole_ref)

    normed = norm_block(rows_ref, gain_ref)
    feature = jnp.dot(normed, whole_ref[1], preferred_element_type=jnp.float32)
    feature = feature.astype(jnp.bfloat16).astype(jnp.float32)
    place = lax.rem(lax.broadcasted_iota(jnp.int32, feature.shape, 0), LEN)
    taps = taps_ref[...]
    tap_count = taps.shape[0]
    summed = None
    for k in range(tap_count):
        amount = tap_count - 1 - k
        moved = shift_down(feature, amount, place, 0.0) if amount else feature
        term = taps[k : k + 1] * moved
        summed = term if summed is None else summed + term
    mixed = summed.astype(jnp.bfloat16)
    recur = jax.nn.sigmoid(jnp.dot(mixed, recur_ref[...], preferred_element_type=jnp.float32))
    inject = jax.nn.sigmoid(jnp.dot(mixed, inject_ref[...], preferred_element_type=jnp.float32))
    log_decay = rate_ref[...] * recur + token_ref[...]
    decay = jnp.exp(log_decay)
    y = 2.0 * log_decay
    series = -y * (
        1.0 + y * (1 / 2) * (1.0 + y * (1 / 3) * (1.0 + y * (1 / 4) * (1.0 + y * (1 / 5) * (1.0 + y * (1 / 6)))))
    )
    loss = jnp.where(y > -0.25, series, 1.0 - decay * decay)
    state = jnp.sqrt(loss) * (inject * mixed.astype(jnp.float32))
    amount = 1
    while amount < LEN:
        state = state + decay * shift_down(state, amount, place, 0.0)
        if 2 * amount < LEN:
            decay = decay * shift_down(decay, amount, place, 1.0)
        amount *= 2
    gate = jnp.dot(normed, whole_ref[0], preferred_element_type=jnp.float32)
    out_ref[...] = (state * jax.nn.gelu(gate)).astype(jnp.bfloat16)


def mixer(owners, full_rows, gain, taps, recur_weight, inject_weight, base_decay_logit, token_log_decay, pieces):
    rows, width = full_rows.shape
    channels = pieces[0].shape[-1]
    rate = -GATE_EXPONENT * jax.nn.softplus(-base_decay_logit)[None, :]
    block = lambda cols: pl.BlockSpec((ROWS, cols), lambda i, *_: (i, 0))
    return pl.pallas_call(
        mixer_kernel,
        grid_spec=pltpu.PrefetchScalarGridSpec(
            num_scalar_prefetch=1,
            grid=(rows // ROWS,),
            in_specs=[
                block(width),
                once((1, width)),
                once(taps.shape),
                once((channels, channels)),
                once((channels, channels)),
                once((1, channels)),
                block(1),
            ]
            + [once(piece.shape) for piece in pieces],
            out_specs=block(channels),
            scratch_shapes=[pltpu.VMEM((2, width, channels), jnp.bfloat16)],
        ),
        out_shape=jax.ShapeDtypeStruct((rows, channels), jnp.bfloat16),
        compiler_params=ORDERED,
        cost_estimate=pl.CostEstimate(
            flops=4 * rows * channels * (channels + width), bytes_accessed=4 * width * channels, transcendentals=0
        ),
    )(
        owners,
        full_rows,
        gain[None],
        taps,
        block_dense(recur_weight),
        block_dense(inject_weight),
        rate,
        token_log_decay[:, None],
        *pieces,
    )


def hidden_kernel(owners_ref, rows_ref, gain_ref, *rest):
    pieces, (out_ref, whole_ref) = rest[:-2], rest[-2:]

    @pl.when(pl.program_id(0) == 0)
    def _():
        collect(owners_ref, pieces, whole_ref)

    normed = norm_block(rows_ref, gain_ref)
    gate = jnp.dot(normed, whole_ref[0], preferred_element_type=jnp.float32)
    up = jnp.dot(normed, whole_ref[1], preferred_element_type=jnp.float32)
    out_ref[...] = (jax.nn.silu(gate) * up).astype(jnp.bfloat16)


def hidden_units(owners, full_rows, gain, pieces):
    rows, width = full_rows.shape
    units = pieces[0].shape[-1]
    block = lambda cols: pl.BlockSpec((ROWS, cols), lambda i, *_: (i, 0))
    return pl.pallas_call(
        hidden_kernel,
        grid_spec=pltpu.PrefetchScalarGridSpec(
            num_scalar_prefetch=1,
            grid=(rows // ROWS,),
            in_specs=[block(width), once((1, width))] + [once(piece.shape) for piece in pieces],
            out_specs=block(units),
            scratch_shapes=[pltpu.VMEM((2, width, units), jnp.bfloat16)],
        ),
        out_shape=jax.ShapeDtypeStruct((rows, units), jnp.bfloat16),
        compiler_params=ORDERED,
        cost_estimate=pl.CostEstimate(
            flops=4 * rows * units * width, bytes_accessed=4 * width * units, transcendentals=0
        ),
    )(owners, full_rows, gain[None], *pieces)


def down_kernel(groups, where_ref, values_ref, *rest):
    pieces, (mine_ref, other_ref) = rest[:-2], rest[-2:]
    values = values_ref[...]
    cols = pieces[0].shape[1]
    width = mine_ref.shape[2]
    y, core = where_ref[len(pieces)], where_ref[len(pieces) + 1]
    for k, piece in enumerate(pieces):
        term = jnp.dot(values, piece[...], preferred_element_type=jnp.float32).astype(jnp.bfloat16)
        start = where_ref[k] * cols
        target = start // width
        offset = pl.multiple_of(lax.rem(start, width), cols)
        turn = lax.rem(target // 2 - y + groups, groups)
        same = lax.rem(target, 2) == core

        @pl.when(same)
        def _():
            mine_ref[turn, :, pl.ds(offset, cols)] = term

        @pl.when(jnp.logical_not(same))
        def _():
            other_ref[turn, :, pl.ds(offset, cols)] = term


def project_down(owners, values, pieces, tp):
    rows, depth = values.shape
    cols = pieces[0].shape[1]
    width = cols * len(pieces) // tp
    groups = tp // 2
    tall = min(rows, 2 * ROWS)
    index = lax.axis_index("tp")
    where = jnp.concatenate([owners, jnp.stack([index // 2, index % 2]).astype(jnp.int32)])
    out_spec = pl.BlockSpec((groups, tall, width), lambda i, *_: (0, i, 0))
    shape = jax.ShapeDtypeStruct((groups, rows, width), jnp.bfloat16)
    return pl.pallas_call(
        functools.partial(down_kernel, groups),
        grid_spec=pltpu.PrefetchScalarGridSpec(
            num_scalar_prefetch=1,
            grid=(rows // tall,),
            in_specs=[pl.BlockSpec((tall, depth), lambda i, *_: (i, 0))] + [once(piece.shape) for piece in pieces],
            out_specs=[out_spec, out_spec],
        ),
        out_shape=[shape, shape],
        compiler_params=ORDERED,
        cost_estimate=pl.CostEstimate(
            flops=2 * rows * depth * cols * len(pieces), bytes_accessed=2 * depth * cols * len(pieces), transcendentals=0
        ),
    )(where, values, *pieces)


def scatter_sum(mine, other, tp):
    groups = tp // 2
    got = lax.ppermute(other, "tp", [(i, i ^ 1) for i in range(tp)])
    widen = lambda value: value.astype(jnp.float32)
    total = None
    for turn in range(1, groups):
        pair = (widen(mine[turn]) + widen(got[turn])).astype(jnp.bfloat16)
        perm = [(i, (i + 2 * turn) % tp) for i in range(tp)]
        arrived = widen(lax.ppermute(pair, "tp", perm))
        total = arrived if total is None else total + arrived
    own = widen(mine[0]) + widen(got[0])
    return own if total is None else own + total


def join_last(pieces):
    return pieces[:-2] + [jnp.concatenate(pieces[-2:], axis=0)]


def shards_general(
    count,
    tp,
    tokens,
    recurrence_norm_gain,
    output_gate_weight,
    recurrence_input_weight,
    convolution_taps,
    recurrence_gate_weight,
    input_gate_weight,
    base_decay_logit,
    token_log_decay,
    recurrence_output_weight,
    feedforward_norm_gain,
    feedforward_gate_weight,
    feedforward_up_weight,
    feedforward_down_weight,
):
    owners = ring_tables(count)
    first = ring_gather(jnp.stack([output_gate_weight, recurrence_input_weight]), count)
    out_pieces = join_last(ring_gather(recurrence_output_weight, count))
    second = ring_gather(jnp.stack([feedforward_gate_weight, feedforward_up_weight]), count)
    down_pieces = join_last(ring_gather(feedforward_down_weight, count))

    full_rows = lax.all_gather(tokens, "tp", axis=1, tiled=True)
    carried = mixer(
        owners,
        full_rows,
        recurrence_norm_gain,
        convolution_taps,
        recurrence_gate_weight,
        input_gate_weight,
        base_decay_logit,
        token_log_decay,
        first,
    )
    mine, other = project_down(owners, carried, out_pieces, tp)
    own_sum = scatter_sum(mine, other, tp)
    residual_own = (tokens.astype(jnp.float32) + own_sum).astype(jnp.bfloat16)
    residual_full = lax.all_gather(residual_own, "tp", axis=1, tiled=True)
    hidden = hidden_units(owners, residual_full, feedforward_norm_gain, second)
    chunks = 2 if hidden.shape[0] % (2 * ROWS) == 0 else 1
    size = hidden.shape[0] // chunks
    sums = []
    for chunk in range(chunks):
        mine, other = project_down(owners, hidden[chunk * size : (chunk + 1) * size], down_pieces, tp)
        sums.append(scatter_sum(mine, other, tp))
    own_down = jnp.concatenate(sums, axis=0)
    return (residual_own.astype(jnp.float32) + own_down).astype(jnp.bfloat16)


LANES = 128
PIECES = 4


def recurrence_block(gate, feature, taps, recur_w, inject_w, rate, token_col):
    feature = feature.astype(jnp.bfloat16).astype(jnp.float32)
    place = lax.rem(lax.broadcasted_iota(jnp.int32, feature.shape, 0), LEN)
    tap_count = taps.shape[0]
    summed = None
    for k in range(tap_count):
        amount = tap_count - 1 - k
        moved = shift_down(feature, amount, place, 0.0) if amount else feature
        term = taps[k : k + 1] * moved
        summed = term if summed is None else summed + term
    mixed = summed.astype(jnp.bfloat16)
    recur = jax.nn.sigmoid(jnp.dot(mixed, recur_w, preferred_element_type=jnp.float32))
    inject = jax.nn.sigmoid(jnp.dot(mixed, inject_w, preferred_element_type=jnp.float32))
    log_decay = rate * recur + token_col
    decay = jnp.exp(log_decay)
    y = 2.0 * log_decay
    series = -y * (
        1.0 + y * (1 / 2) * (1.0 + y * (1 / 3) * (1.0 + y * (1 / 4) * (1.0 + y * (1 / 5) * (1.0 + y * (1 / 6)))))
    )
    loss = jnp.where(y > -0.25, series, 1.0 - decay * decay)
    state = jnp.sqrt(loss) * (inject * mixed.astype(jnp.float32))
    amount = 1
    while amount < LEN:
        state = state + decay * shift_down(state, amount, place, 0.0)
        if 2 * amount < LEN:
            decay = decay * shift_down(decay, amount, place, 1.0)
        amount *= 2
    return (state * jax.nn.gelu(gate)).astype(jnp.bfloat16)


def layer_kernel(
    planes,
    tokens_ref,
    token_ref,
    gate_in_ref,
    feature_in_ref,
    out_w_ref,
    gate_up_ref,
    up_ref,
    down_ref,
    gain_ref,
    gain_two_ref,
    taps_ref,
    recur_ref,
    inject_ref,
    rate_ref,
    result_ref,
    rows_ref,
    resid_ref,
    wf_ref,
    wo_ref,
    wg_ref,
    wd_ref,
    hid_ref,
    keep_ref,
    csend_ref,
    crecv_ref,
    xrecv_ref,
    ysend_ref,
    yrecv_ref,
    tokd_ref,
    chan_ref,
    local_sem,
    raw_sem,
    token_sem,
    wx_sem,
    wz_sem,
    wr_sem,
    ags_sem,
    agr_sem,
    cs_sem,
    cr_sem,
    xs_sem,
    xr_sem,
    ys_sem,
    yr_sem,
    dcs_sem,
    dcr_sem,
    dxs_sem,
    dxr_sem,
    dys_sem,
    dyr_sem,
):
    fs, tp = lax.axis_index("fs"), lax.axis_index("tp")
    z, x = fs // 2, lax.rem(fs, 2)
    yy, c = tp // 2, lax.rem(tp, 2)
    ox, oy, oc = 1 - x, 1 - yy, 1 - c
    here = (fs, tp)
    to_x, to_y, to_c = (z * 2 + ox, tp), (fs, oy * 2 + c), (fs, yy * 2 + oc)
    to_z = ((fs + 2, tp), (fs - 2, tp))
    last = planes - 1
    held, cols = tokens_ref.shape
    depth_rows = gate_in_ref.shape[2]
    chans = wo_ref.shape[0]
    units = wd_ref.shape[0]
    chunks = held // ROWS

    def mo(value, step):
        return pl.multiple_of(value, step)

    def remote(src, dst, send, recv, dest):
        return pltpu.make_async_remote_copy(
            src_ref=src, dst_ref=dst, send_sem=send, recv_sem=recv, device_id=dest, device_id_type=pl.DeviceIdType.MESH
        )

    staged = resid_ref.at[0:depth_rows, : 2 * units]
    raw = [resid_ref.at[n * depth_rows : (n + 1) * depth_rows, : 2 * units] for n in range(1, 3)]
    sources = (None, out_w_ref, None, down_ref)

    def block(g, s):
        spot = pl.ds(mo(s * depth_rows, depth_rows), depth_rows)
        if g == 0:
            return wf_ref.at[:, spot]
        if g == 1:
            return wo_ref.at[:, spot]
        if g == 2:
            return wg_ref.at[spot, :]
        return wd_ref.at[:, spot]

    def z_copy(g, s, way, src=None):
        dst = block(g, s)
        return remote(dst if src is None else src, dst, wz_sem.at[way, g, s], wr_sem.at[g, s], to_z[way])

    def x_copy(g):
        src = staged if g == 2 else sources[g].at[ox]
        return remote(src, block(g, fs), wx_sem.at[g], wr_sem.at[g, fs], to_x)

    projections = (gate_in_ref, feature_in_ref)

    def first_spot(n):
        return wf_ref.at[n * chans : (n + 1) * chans, pl.ds(mo(fs * depth_rows, depth_rows), depth_rows)]

    def first_x_copy(n):
        return remote(projections[n].at[ox], first_spot(n), wx_sem.at[4 * n], wr_sem.at[0, fs], to_x)

    def first_local_copy(n):
        return pltpu.make_async_copy(projections[n].at[x], first_spot(n), local_sem.at[2 * n])

    def local_copy(g):
        return pltpu.make_async_copy(sources[g].at[x], block(g, fs), local_sem.at[g])

    def z_send(g, s, src=None):
        @pl.when(z < last)
        def _():
            z_copy(g, s, 0, src).start()

        @pl.when(z > 0)
        def _():
            z_copy(g, s, 1, src).start()

    def z_send_far(g, s):
        @pl.when(z < planes // 2)
        def _():
            z_copy(g, s, 0).start()

        @pl.when(z >= planes // 2)
        def _():
            z_copy(g, s, 1).start()

    def z_send_near(g, s):
        @pl.when((z > 0) & (z < planes // 2))
        def _():
            z_copy(g, s, 1).start()

        @pl.when((z < last) & (z >= planes // 2))
        def _():
            z_copy(g, s, 0).start()

    def x_forward(g):
        s = z * 2 + ox
        z_copy(g, s, 0).wait_recv()
        z_send(g, s)

    def z_pass(g, d, sides):
        @pl.when((z > 0) & (z < last))
        def _():
            for side in sides:

                @pl.when(z - d >= 0)
                def _():
                    s = (z - d) * 2 + side
                    z_copy(g, s, 0).wait_recv()
                    z_copy(g, s, 0).start()

                @pl.when(z + d <= last)
                def _():
                    s = (z + d) * 2 + side
                    z_copy(g, s, 1).wait_recv()
                    z_copy(g, s, 1).start()

    def z_end(g, d, sides):
        for side in sides:

            @pl.when((z == last) & (z - d >= 0))
            def _():
                z_copy(g, (z - d) * 2 + side, 0).wait_recv()

            @pl.when((z == 0) & (z + d <= last))
            def _():
                z_copy(g, (z + d) * 2 + side, 1).wait_recv()

    def z_end_all(g):
        for d in range(1, planes):
            z_end(g, d, both)

    both = (x, ox)
    fixed = (0, 1)

    def z_drain(g):
        for way in range(2):

            @pl.loop(0, 2 * planes)
            def _(s):
                sent = (s // 2 <= z) & (z < last) if way == 0 else (s // 2 >= z) & (z > 0)

                @pl.when(sent)
                def _():
                    z_copy(g, s, way).wait_send()

    def spread(buf, phase, k, slot, at, dest):
        xi, yi, ci = at
        where = buf.at[
            pl.ds(mo(xi * held + k * ROWS, ROWS), ROWS), pl.ds(mo((yi * 2 + ci) * cols, cols), cols)
        ]
        return remote(
            where, where, ags_sem.at[phase, k, slot], agr_sem.at[phase, k, xi * 4 + yi * 2 + ci], dest
        )

    own = (x, yy, c)

    def spread_own(buf, phase, k):
        spread(buf, phase, k, 0, own, to_x).start()
        spread(buf, phase, k, 1, own, to_y).start()
        spread(buf, phase, k, 2, own, to_c).start()

    def routes(swap):
        over_x, over_y = (ox, yy, c), (x, oy, c)
        return (over_y, over_x, to_x) if swap else (over_x, over_y, to_y)

    def spread_on(buf, phase, k, swap):
        at, _, dest = routes(swap)
        spread(buf, phase, k, 3, at, dest).wait_recv()
        spread(buf, phase, k, 3, at, dest).start()
        spread(buf, phase, k, 4, at, to_c).start()

    def spread_rest(buf, phase, k, swap):
        _, other, _ = routes(swap)
        for slot, at in ((5, other), (6, (ox, oy, c))):
            spread(buf, phase, k, slot, at, to_c).wait_recv()
            spread(buf, phase, k, slot, at, to_c).start()

    def spread_c(buf, phase, k):
        for xi in (x, ox):
            for yi in (yy, oy):
                spread(buf, phase, k, 2, (xi, yi, oc), to_c).wait_recv()

    def spread_drain(buf, phase, k, swap):
        at, other, dest = routes(swap)
        spread(buf, phase, k, 0, own, to_x).wait_send()
        spread(buf, phase, k, 1, own, to_y).wait_send()
        spread(buf, phase, k, 2, own, to_c).wait_send()
        spread(buf, phase, k, 3, at, dest).wait_send()
        spread(buf, phase, k, 4, at, to_c).wait_send()
        spread(buf, phase, k, 5, other, to_c).wait_send()
        spread(buf, phase, k, 6, (ox, oy, c), to_c).wait_send()

    def tall(j):
        return pl.ds(mo(j * ROWS, ROWS), ROWS)

    def c_copy(j):
        return remote(csend_ref.at[tall(j), :], crecv_ref.at[tall(j), :], cs_sem.at[j], cr_sem.at[j], to_c)

    split = chunks // 2

    def side_cols(side):
        return pl.ds(mo(side * cols, cols), cols)

    def x_sum_copy(k):
        return remote(keep_ref.at[tall(k), :], xrecv_ref.at[tall(k), :], xs_sem.at[k], xr_sem.at[k], to_x)

    def y_sum_copy(k):
        return remote(ysend_ref.at[tall(k), :], yrecv_ref.at[tall(k), :], ys_sem.at[k], yr_sem.at[k], to_y)

    def y_own_copy(k):
        src = keep_ref.at[tall(chunks + k), side_cols(oy)]
        return remote(src, yrecv_ref.at[tall(k), :], ys_sem.at[k], yr_sem.at[k], to_y)

    def y_across_copy(k):
        src = keep_ref.at[tall(k), side_cols(oy)]
        return remote(src, ysend_ref.at[tall(k), :], ys_sem.at[chunks + k], yr_sem.at[chunks + k], to_y)

    def x_half_copy(k):
        spot = side_cols(yy)
        return remote(
            keep_ref.at[tall(k), spot], xrecv_ref.at[tall(k), spot], xs_sem.at[k], xr_sem.at[k], to_x
        )

    def chunk_rows(j):
        side = jnp.where(j < chunks, ox, x)
        k = lax.rem(j, chunks)
        return side, k, pl.ds(mo(side * held + k * ROWS, ROWS), ROWS)

    def produce(j, left, weight_ref):
        for half in range(2):
            spot = pl.ds(mo((half * 2 + oc) * cols, cols), cols)
            part = jnp.dot(left, weight_ref[:, spot], preferred_element_type=jnp.float32)
            csend_ref[tall(j), half * cols : (half + 1) * cols] = part.astype(jnp.bfloat16)
        for half in range(2):
            spot = pl.ds(mo((half * 2 + c) * cols, cols), cols)
            part = jnp.dot(left, weight_ref[:, spot], preferred_element_type=jnp.float32)
            keep_ref[tall(j), half * cols : (half + 1) * cols] = part.astype(jnp.bfloat16)
        c_copy(j).start()

    def join_cores(j):
        c_copy(j).wait_recv()
        keep_ref[tall(j), :] = (
            keep_ref[tall(j), :].astype(jnp.float32) + crecv_ref[tall(j), :].astype(jnp.float32)
        ).astype(jnp.bfloat16)

        @pl.when(j < split)
        def _():
            x_sum_copy(j).start()

        @pl.when((j >= split) & (j < chunks))
        def _():
            y_across_copy(j).start()

        @pl.when(j >= chunks + split)
        def _():
            y_own_copy(j - chunks).start()

    def turn(i):
        across = lax.rem(i, 2) * split + i // 2
        mine = chunks + lax.rem(i - chunks + split + chunks, chunks)
        return jnp.where(i < chunks, across, mine)

    def produce_all():
        @pl.loop(0, 2 * chunks)
        def _(i):
            j = turn(i)
            _, _, rows = chunk_rows(j)
            produce(j, hid_ref[rows, :chans], wo_ref)

            @pl.when(i > 0)
            def _():
                join_cores(turn(i - 1))

        join_cores(turn(2 * chunks - 1))

    def halves(k, side):
        spot = side_cols(side)
        return keep_ref[tall(chunks + k), spot].astype(jnp.float32) + xrecv_ref[tall(k), spot].astype(jnp.float32)

    def join_x(k):
        x_sum_copy(k).wait_recv()
        ysend_ref[tall(k), :] = halves(k, oy).astype(jnp.bfloat16)
        y_sum_copy(k).start()

    def join_across(k):
        y_across_copy(k).wait_recv()
        spot = side_cols(yy)
        keep_ref[tall(k), spot] = (
            keep_ref[tall(k), spot].astype(jnp.float32) + ysend_ref[tall(k), :].astype(jnp.float32)
        ).astype(jnp.bfloat16)
        x_half_copy(k).start()

    def join_y(k):
        if k < split:
            y_sum_copy(k).wait_recv()
        else:
            y_own_copy(k).wait_recv()
            x_half_copy(k).wait_recv()
        return halves(k, yy) + yrecv_ref[tall(k), :].astype(jnp.float32)

    def sums_drain():
        for j in range(2 * chunks):
            c_copy(j).wait_send()
        for k in range(chunks):
            if k < split:
                x_sum_copy(k).wait_send()
                y_sum_copy(k).wait_send()
            else:
                y_own_copy(k).wait_send()
                y_across_copy(k).wait_send()
                x_half_copy(k).wait_send()

    def near(n):
        orders = [sorted(range(planes), key=lambda other: (abs(other - p), other)) for p in range(planes)]
        found = orders[0][n]
        for p in range(1, planes):
            found = jnp.where(z == p, orders[p][n], found)
        return found

    x_rows = pl.ds(mo(ox * held, held), held)
    own_rows = pl.ds(mo(x * held, held), held)

    def wide_cols(zi, xi):
        return pl.ds(mo((zi * 2 + xi) * depth_rows, depth_rows), depth_rows)

    def slot_cols(zi, xi):
        return pl.ds(mo((zi // 2 * 2 + xi) * depth_rows, depth_rows), depth_rows)

    def down_c_copy(zi, xi, half):
        rows = own_rows if half else x_rows
        at = zi * 2 + xi
        return remote(
            rows_ref.at[rows, wide_cols(zi, xi)],
            crecv_ref.at[rows, slot_cols(zi, xi)],
            dcs_sem.at[half, at],
            dcr_sem.at[half, at],
            to_c,
        )

    piece = held // PIECES

    def piece_rows(side, p):
        return pl.ds(mo(side * held + p * piece, piece), piece)

    def down_x_copy(zi, xi, p):
        at = zi * 2 + xi
        return remote(
            rows_ref.at[piece_rows(ox, p), wide_cols(zi, xi)],
            xrecv_ref.at[p * piece : (p + 1) * piece, slot_cols(zi, xi)],
            dxs_sem.at[p, at],
            dxr_sem.at[p, at],
            to_x,
        )

    def down_y_copy(zi, xi, p):
        return remote(
            rows_ref.at[piece_rows(x, p), wide_cols(zi, xi)],
            yrecv_ref.at[p * piece : (p + 1) * piece, xi * depth_rows : (xi + 1) * depth_rows],
            dys_sem.at[p, xi],
            dyr_sem.at[p, xi],
            to_y,
        )

    def lower(zi, xi, half):
        rows = own_rows if half else x_rows
        part = jnp.dot(hid_ref[rows, :], wd_ref[:, wide_cols(zi, xi)], preferred_element_type=jnp.float32)
        rows_ref[rows, wide_cols(zi, xi)] = part.astype(jnp.bfloat16)

        @pl.when(lax.rem(zi, 2) == oc)
        def _():
            down_c_copy(zi, xi, half).start()

    def gather(zi, xi, half):
        @pl.when(lax.rem(zi, 2) == c)
        def _():
            down_c_copy(zi, xi, half).wait_recv()
            for p in range(PIECES):
                rows = piece_rows(x if half else ox, p)
                rows_ref[rows, wide_cols(zi, xi)] = (
                    rows_ref[rows, wide_cols(zi, xi)].astype(jnp.float32)
                    + crecv_ref[rows, slot_cols(zi, xi)].astype(jnp.float32)
                ).astype(jnp.bfloat16)
                if half == 0:
                    down_x_copy(zi, xi, p).start()

    def both_x(zi, xi, p):
        mine = rows_ref[piece_rows(x, p), wide_cols(zi, xi)].astype(jnp.float32)
        return mine + xrecv_ref[p * piece : (p + 1) * piece, slot_cols(zi, xi)].astype(jnp.float32)

    def down_join_x(zi, xi):
        @pl.when(lax.rem(zi, 2) == c)
        def _():
            for p in range(PIECES):
                down_x_copy(zi, xi, p).wait_recv()

                @pl.when(zi // 2 == oy)
                def _():
                    rows_ref[piece_rows(x, p), wide_cols(zi, xi)] = both_x(zi, xi, p).astype(jnp.bfloat16)
                    down_y_copy(zi, xi, p).start()

    def down_last(zi, xi):
        @pl.when(zi == tp)
        def _():
            for p in range(PIECES):
                down_y_copy(zi, xi, p).wait_recv()
                rows = slice(p * piece, (p + 1) * piece)
                spot = slice(xi * depth_rows, (xi + 1) * depth_rows)
                total = both_x(zi, xi, p) + yrecv_ref[rows, spot].astype(jnp.float32)
                total = total + resid_ref[piece_rows(x, p), wide_cols(zi, xi)].astype(jnp.float32)
                result_ref[rows, spot] = total.astype(jnp.bfloat16)

    def down_drain_c(zi, xi):
        @pl.when(lax.rem(zi, 2) == oc)
        def _():
            for half in range(2):
                down_c_copy(zi, xi, half).wait_send()

    def down_drain(zi, xi):
        @pl.when(lax.rem(zi, 2) == c)
        def _():
            for p in range(PIECES):
                down_x_copy(zi, xi, p).wait_send()

            @pl.when(zi // 2 == oy)
            def _():
                for p in range(PIECES):
                    down_y_copy(zi, xi, p).wait_send()

    own_cols = pl.ds(mo(tp * cols, cols), cols)

    def own_spot(k):
        return pl.ds(mo(x * held + k * ROWS, ROWS), ROWS)

    barrier = pltpu.get_barrier_semaphore()
    for dest in (to_x, to_y, to_c):
        pl.semaphore_signal(barrier, inc=1, device_id=dest, device_id_type=pl.DeviceIdType.MESH)

    @pl.when(z < last)
    def _():
        pl.semaphore_signal(barrier, inc=1, device_id=to_z[0], device_id_type=pl.DeviceIdType.MESH)

    @pl.when(z > 0)
    def _():
        pl.semaphore_signal(barrier, inc=1, device_id=to_z[1], device_id_type=pl.DeviceIdType.MESH)

    own_tokens = pltpu.make_async_copy(
        tokens_ref, rows_ref.at[pl.ds(mo(x * held, held), held), own_cols], token_sem.at[0]
    )
    own_decay = pltpu.make_async_copy(token_ref, tokd_ref.at[x], token_sem.at[1])
    sent_decay = remote(token_ref, tokd_ref.at[x], token_sem.at[2], token_sem.at[3], to_x)
    own_tokens.start()
    own_decay.start()
    raws = [
        pltpu.make_async_copy(source, target, raw_sem.at[n])
        for n, (source, target) in enumerate(zip((gate_up_ref, up_ref), raw))
    ]
    for n in range(2):
        first_local_copy(n).start()
    for copy in raws:
        copy.start()
    for g in (1, 3):
        local_copy(g).start()
    first_half = x == 0

    def pick(values, here, width):
        left, right = values[:, :width], values[:, width:]
        return jnp.where(first_half == here, left, right)

    for n in range(2):
        first_local_copy(n).wait()
    pl.semaphore_wait(barrier, 3 + (z < last).astype(jnp.int32) + (z > 0).astype(jnp.int32))

    for n in range(2):
        first_x_copy(n).start()
    z_send(0, fs)
    z_send(1, fs, sources[1].at[x])
    sent_decay.start()
    own_tokens.wait()
    for k in range(chunks):
        spread_own(rows_ref, 0, k)
        if k == 0:
            x_copy(1).start()
    raws[0].wait()
    raws[1].wait()
    own_second = block(2, fs)
    for n in range(2):
        values = raw[n][...]
        for here, target in ((True, own_second), (False, staged)):
            target[:, n * units : (n + 1) * units] = pick(values, here, units)
    x_copy(2).start()
    x_copy(3).start()
    chan_ref[0 : taps_ref.shape[0], :] = jnp.where(first_half, taps_ref[:, :chans], taps_ref[:, chans:])
    chan_ref[taps_ref.shape[0] : taps_ref.shape[0] + 1, :] = jnp.where(
        first_half, rate_ref[:, :chans], rate_ref[:, chans:]
    )
    x_forward(0)
    z_pass(0, 1, both)
    x_forward(1)
    for k in range(chunks):
        spread_on(rows_ref, 0, k, False)
    z_pass(0, 2, both)
    z_pass(1, 1, both)
    for k in range(chunks):
        spread_rest(rows_ref, 0, k, False)
    for k in range(chunks):
        spread_c(rows_ref, 0, k)
    for g in (1, 3):
        local_copy(g).wait()
    own_decay.wait()
    sent_decay.wait()
    z_end_all(0)

    def mix(start):
        @pl.loop(start, start + chunks)
        def _(j):
            side, k, rows = chunk_rows(j)
            normed = norm_block(rows_ref.at[rows, :], gain_ref)
            prod = lax.dot_general(
                normed, wf_ref[...], (((1,), (1,)), ((), ())), preferred_element_type=jnp.float32
            )
            columns = []
            for n in range(ROWS // LEN):
                line = tokd_ref[side, pl.ds(k * (ROWS // LEN) + n, 1), :]
                columns.append(jnp.transpose(jnp.broadcast_to(line, (LEN, LANES))))
            column = jnp.concatenate(columns, axis=0)
            column = jnp.concatenate([column] * (-(-chans // LANES)), axis=1)[:, :chans]
            taps = chan_ref[0 : taps_ref.shape[0], :]
            rate = chan_ref[taps_ref.shape[0] : taps_ref.shape[0] + 1, :]
            hid_ref[rows, :chans] = recurrence_block(
                prod[:, :chans], prod[:, chans:], taps, recur_ref[x], inject_ref[x], rate, column
            )

    mix(0)
    z_pass(1, 2, both)
    z_send(2, fs)
    x_forward(2)
    mix(chunks)
    z_end_all(1)
    x_copy(2).wait_send()
    produce_all()

    def residual_chunk(k):
        total = join_y(k) + rows_ref[own_spot(k), own_cols].astype(jnp.float32)
        resid_ref[own_spot(k), own_cols] = total.astype(jnp.bfloat16)
        spread_own(resid_ref, 1, k)

    for k in range(split, chunks):
        join_across(k)
    z_pass(2, 1, (x,))
    for k in range(split):
        join_x(k)
    z_pass(2, 1, (ox,))
    weave = [k + side for k in range(split) for side in (split, 0)]
    for k in weave:
        residual_chunk(k)
    z_pass(2, 2, (x,))
    z_copy(3, z * 2 + ox, 0).wait_recv()
    for xi in range(2):
        z_send_far(3, z * 2 + xi)
    for k in weave:
        spread_on(resid_ref, 1, k, k % 2 == 1)
    z_pass(2, 2, (ox,))
    for k in weave:
        spread_rest(resid_ref, 1, k, k % 2 == 1)
    for k in range(chunks):
        spread_c(resid_ref, 1, k)
    sums_drain()
    for k in range(chunks):
        spread_drain(rows_ref, 0, k, False)
    z_end_all(2)

    def hide(start, stop):
        @pl.loop(start, stop)
        def _(j):
            _, _, rows = chunk_rows(j)
            normed = norm_block(resid_ref.at[rows, :], gain_two_ref)
            pair = jnp.dot(normed, wg_ref[...], preferred_element_type=jnp.float32)
            hid_ref[rows, :] = (jax.nn.silu(pair[:, :units]) * pair[:, units:]).astype(jnp.bfloat16)

    def half_sums(n, half):
        for xi in range(2):
            lower(near(n), xi, half)
        for xi in range(2):
            gather(near(n), xi, half)

    def join_one(n, xi):
        down_join_x(near(n), xi)

    def lower_one(n, xi, half):
        lower(near(n), xi, half)

    def gather_one(n, xi, half):
        gather(near(n), xi, half)

    hide(0, chunks)
    for xi in range(2):
        z_send_near(3, z * 2 + xi)
    half_sums(0, 0)
    z_pass(3, 1, fixed)
    hide(chunks, chunks + split)
    z_end(3, 1, fixed)
    half_sums(1, 0)
    hide(chunks + split, 2 * chunks)
    for n in range(2):
        for xi in range(2):
            lower_one(n, xi, 1)
    z_pass(3, 2, fixed)
    z_end(3, 2, (0,))
    lower_one(2, 0, 0)
    for n in range(2):
        for xi in range(2):
            gather_one(n, xi, 1)
    gather_one(2, 0, 0)
    lower_one(2, 0, 1)
    for xi in range(2):
        join_one(0, xi)
    z_end(3, 2, (1,))
    lower_one(2, 1, 0)
    lower_one(2, 1, 1)
    gather_one(2, 1, 0)
    gather_one(2, 0, 1)
    gather_one(2, 1, 1)
    for xi in range(2):
        join_one(1, xi)
    z_end(3, 3, (0,))
    join_one(2, 0)
    lower_one(3, 0, 0)
    lower_one(3, 0, 1)
    gather_one(3, 0, 0)
    gather_one(3, 0, 1)
    for n in range(2):
        first_x_copy(n).wait_send()
    for g in (1, 3):
        x_copy(g).wait_send()
    for g in range(3):
        z_drain(g)
    for k in range(chunks):
        spread_drain(resid_ref, 1, k, k % 2 == 1)
    for n in range(3):
        for xi in range(2):
            down_drain_c(near(n), xi)
    z_end(3, 3, (1,))
    lower_one(3, 1, 0)
    lower_one(3, 1, 1)
    gather_one(3, 1, 0)
    join_one(2, 1)
    join_one(3, 0)
    gather_one(3, 1, 1)
    join_one(3, 1)
    for n in range(planes):
        for xi in range(2):
            down_last(near(n), xi)

    for xi in range(2):
        down_drain_c(near(3), xi)
    for n in range(planes):
        for xi in range(2):
            down_drain(near(n), xi)
    z_drain(3)


def shards_fused(
    count,
    tp,
    tokens,
    recurrence_norm_gain,
    output_gate_weight,
    recurrence_input_weight,
    convolution_taps,
    recurrence_gate_weight,
    input_gate_weight,
    base_decay_logit,
    token_log_decay,
    recurrence_output_weight,
    feedforward_norm_gain,
    feedforward_gate_weight,
    feedforward_up_weight,
    feedforward_down_weight,
):
    planes = count // 2
    held, cols = tokens.shape
    width = cols * tp
    chans = output_gate_weight.shape[1] // 2
    units = feedforward_gate_weight.shape[1] // 2
    chunks = held // ROWS

    out_w = recurrence_output_weight.reshape(2, chans, -1)
    down = feedforward_down_weight.reshape(2, units, -1)
    rate = -GATE_EXPONENT * jax.nn.softplus(-base_decay_logit)[None, :]
    anywhere = pl.BlockSpec(memory_space=pl.ANY)
    inside = pl.BlockSpec(memory_space=pltpu.VMEM)
    bf16 = jnp.bfloat16
    copies = pltpu.SemaphoreType.DMA
    flops = 2 * 2 * held * (width * (2 * chans + 2 * units) + width * (chans + units))
    return pl.pallas_call(
        functools.partial(layer_kernel, planes),
        in_specs=[anywhere] * 8 + [inside] * 6,
        out_specs=inside,
        out_shape=jax.ShapeDtypeStruct((held, cols), bf16),
        scratch_shapes=[
            pltpu.VMEM((2 * held, width), bf16),
            pltpu.VMEM((2 * held, width), bf16),
            pltpu.VMEM((2 * chans, width), bf16),
            pltpu.VMEM((chans, width), bf16),
            pltpu.VMEM((width, 2 * units), bf16),
            pltpu.VMEM((units, width), bf16),
            pltpu.VMEM((2 * held, units), bf16),
            pltpu.VMEM((2 * held, 2 * cols), bf16),
            pltpu.VMEM((2 * held, 2 * cols), bf16),
            pltpu.VMEM((2 * held, 2 * cols), bf16),
            pltpu.VMEM((held, 2 * cols), bf16),
            pltpu.VMEM((held, cols), bf16),
            pltpu.VMEM((held, cols), bf16),
            pltpu.VMEM((2, held // LEN, LEN), jnp.float32),
            pltpu.VMEM((convolution_taps.shape[0] + 1, chans), jnp.float32),
            copies((4,)),
            copies((2,)),
            copies((4,)),
            copies((5,)),
            copies((2, 4, 2 * planes)),
            copies((4, 2 * planes)),
            copies((2, chunks, 7)),
            copies((2, chunks, 8)),
            copies((2 * chunks,)),
            copies((2 * chunks,)),
            copies((chunks,)),
            copies((chunks,)),
            copies((2 * chunks,)),
            copies((2 * chunks,)),
            copies((2, 2 * planes)),
            copies((2, 2 * planes)),
            copies((PIECES, 2 * planes)),
            copies((PIECES, 2 * planes)),
            copies((PIECES, 2)),
            copies((PIECES, 2)),
        ],
        compiler_params=pltpu.CompilerParams(
            collective_id=0, has_side_effects=True, vmem_limit_bytes=63 * 1024 * 1024
        ),
        cost_estimate=pl.CostEstimate(flops=flops, bytes_accessed=8 * held * width, transcendentals=0),
    )(
        tokens,
        token_log_decay.reshape(held // LEN, LEN),
        output_gate_weight.T.reshape(2, chans, -1),
        recurrence_input_weight.T.reshape(2, chans, -1),
        out_w,
        feedforward_gate_weight,
        feedforward_up_weight,
        down,
        recurrence_norm_gain[None],
        feedforward_norm_gain[None],
        convolution_taps,
        recurrence_gate_weight,
        input_gate_weight,
        rate,
    )


def solution(mesh):
    in_specs = (
        P("fs", "tp"),
        P(),
        P("fs", "tp"),
        P("fs", "tp"),
        P(None, "tp"),
        P("tp", None, None),
        P("tp", None, None),
        P("tp"),
        P("fs"),
        P("tp", "fs"),
        P(),
        P("fs", "tp"),
        P("fs", "tp"),
        P("tp", "fs"),
    )
    count, tp = mesh.shape["fs"], mesh.shape["tp"]
    if tp == 4:
        body = functools.partial(shards_fused, count, tp)
        return jax.shard_map(body, mesh=mesh, in_specs=in_specs, out_specs=P("fs", "tp"), check_vma=False)
    body = functools.partial(shards_general, count, tp)
    return jax.shard_map(body, mesh=mesh, in_specs=in_specs, out_specs=P("fs", "tp"), check_vma=False)
```
